32 devices in a mesh: ep: 8 (over z, x), tp: 4 (over y, core).
Axes of the slice: x: 2, y: 2, z: 4, core: 2. Of those that a mesh axis runs over, the one named last changes fastest.
Arguments:
- queries: bfloat16 [8192, 2048], P('ep', 'tp'), may hold values from -128 to 128
- key_heads: bfloat16 [8192, 1024], P('ep', 'tp'), may hold values from -6 to 6
- value_heads: bfloat16 [8192, 1024], P('ep', 'tp'), may hold values from -6 to 6
- sink_logits: float32 [32], P('tp'), may hold values from 1 to 5
- mix_weight: bfloat16 [2048, 2048], replicated, may hold values from -1 to 1
- expert_input: bfloat16 [4096, 2048], P(('ep', 'tp')), may hold values from -6 to 6
- norm_gain: float32 [2048], replicated, may hold values from 0.1 to 1.9
- routes: int32 [4096, 4], P(('ep', 'tp')), may hold values from 0 to 31, all different within a row; in each aligned block of 128 rows (0 to 127, 128 to 255, ...) at most 32 rows name the same one
- route_weights: float32 [4096, 4], P(('ep', 'tp')), may hold values from 0.1 to 1
- gate_weight: bfloat16 [32, 2048, 1024], P(('ep', 'tp')), may hold values from -0.375 to 0.375
- up_weight: bfloat16 [32, 2048, 1024], P(('ep', 'tp')), may hold values from -0.375 to 0.375
- down_weight: bfloat16 [32, 1024, 2048], P(('ep', 'tp')), may hold values from -0.046875 to 0.046875
Outputs:
- mixer_out: bfloat16 [8192, 2048], P(('ep', 'tp'))
- experts_out: bfloat16 [4096, 2048], P(('ep', 'tp'))
The draws below stay inside these ranges and needn't reach their ends.
Inputs may be any that keep to these rules, and one draw needn't show every extreme that they name: `routes`: each row names 4 different experts; within the 128 rows of one device no expert is named more than 32 times, and in some devices' rows some expert is named exactly 32 times.
All inputs are finite; a program needn't handle non-finite values.
Results may differ from the reference program's by a relative error of at most 0.012.
The reference program's roundings to bfloat16 on the way count: a program that leaves them out, or rounds other values in their place, can miss the bound.
Values may be sent and summed in bfloat16 or wider, within the bound.
A program may use at most 128 MiB of HBM per device.

```python
import math
import jax
import jax.numpy as jnp
import numpy as np
from jax import lax

D = 2048
HEADS = 32
KV_HEADS = 16
HEAD_DIM = 64
WINDOW = 128
GRID_W = 64
FF = 1024
TOPK = 4
TOK_B = 128
TOKENS_A = 8192
TOKENS_B = 4096
EXPERTS = 32
CAP = 32
N_EP = 8
N_TP = 4


def query_key_pair(key):
    base_seed = jax.random.fold_in(key, 7)
    query_seed, key_seed = jax.random.split(base_seed, 2)
    length = TOKENS_A
    key_part = jnp.clip(jax.random.normal(key_seed, (length, KV_HEADS * HEAD_DIM), jnp.float32), -4.0, 4.0)
    query_part = jnp.clip(jax.random.normal(query_seed, (length, HEADS * HEAD_DIM), jnp.float32), -4.0, 4.0)
    return (query_part, key_part)


def draw_queries(key, part):
    return query_key_pair(key)[0].astype(jnp.bfloat16)


def draw_key_heads(key, part):
    return query_key_pair(key)[1].astype(jnp.bfloat16)


def level_of(own_key, extent, pieces, least, top_value):
    gain = 1.0
    for position, blocks in pieces:
        draws = jax.random.uniform(jax.random.fold_in(jax.random.fold_in(own_key, 6), position), (blocks,), jnp.float32, least / len(pieces), top_value / len(pieces))
        gain = gain * jnp.repeat(jnp.exp(draws), extent[position] // blocks).reshape((-1,) + (1,) * (len(extent) - 1 - position))
    return gain


def routed_block(stream_key, own, number, rows, number_of, top, bound, slope):
    sequence = jax.random.permutation(stream_key, number_of)
    heavy_load, usual = shares(number_of, rows * top, bound, slope, True), shares(number_of, rows * top, bound, slope, False)
    places = jnp.arange(number_of)

    def named(lengths, turn):
        used = int((lengths > 0).sum())
        fixed = max(1, used // 4)
        shifted = fixed + (places - fixed + turn * (used - fixed)) % max(1, number_of - fixed)
        return jnp.zeros((number_of,), jnp.int32).at[sequence[jnp.where(places < fixed, places, shifted)]].set(jnp.asarray(lengths, jnp.int32))

    lengths = jnp.where(number % 4 == 0, named(heavy_load, number // 4), named(usual, number - number // 4 - 1))
    mixed = jax.random.permutation(jax.random.fold_in(own, 3), number_of)
    giver, taker = mixed[0:number_of // 2 * 2:2], mixed[1:number_of // 2 * 2:2]
    room = jnp.minimum(lengths[giver] - 1, bound - lengths[taker]) // 2
    room = jnp.where((giver == sequence[0]) | (taker == sequence[0]) | (lengths[taker] == 0), 0, jnp.maximum(room, 0))
    shifted = jax.random.randint(jax.random.fold_in(own, 4), (number_of // 2,), 0, 1 << 20) % (room + 1)
    lengths = lengths.at[giver].add(-shifted).at[taker].add(shifted)
    items = jnp.searchsorted(jnp.cumsum(lengths), jnp.arange(rows * top), side="right").astype(jnp.int32)
    table = items.reshape(top, rows).T
    table = table[jax.random.permutation(jax.random.fold_in(own, 1), rows)]
    turn = jax.random.randint(jax.random.fold_in(own, 2), (rows, 1), 0, top)
    return jnp.take_along_axis(table, (jnp.arange(top)[None, :] + turn) % top, axis=1)


def shares(count, total, most, skew, full):
    loads = [(1 << 20) // math.isqrt(rank ** skew) + 1 for rank in range(1, count + 1)]
    largest = most if full else min(most, max(-(-total // count), total * loads[0] // sum(loads)))
    least = 1 if total - largest >= count - 1 else 0
    counts, rest = [largest] + [least] * (count - 1), total - largest - least * (count - 1)
    while rest > 0:
        candidates = [i for i in range(1, count) if counts[i] < largest] or [i for i in range(1, count) if counts[i] < most]
        whole, budget = sum([loads[i] for i in candidates]), rest
        for i in candidates:
            extra = min(most - counts[i], max(1, budget * loads[i] // whole), rest)
            counts[i] = counts[i] + extra
            rest = rest - extra
    return np.array(counts)


def scatter_about(key, extent, scale, reach, shards=(), kind=jnp.bfloat16):
    result = scale * jax.random.normal(key, extent, jnp.float32)
    if shards:
        result = result * level_of(key, extent, shards, -0.22, 0.18)
    return jnp.clip(result, -reach, reach).astype(kind)


def setup_inputs(seed: int = 0) -> dict:
    key_list = jax.random.split(jax.random.key(seed), 13)
    queries = draw_queries(jax.random.fold_in(key_list[12], 71), 0)
    key_heads = draw_key_heads(jax.random.fold_in(key_list[12], 71), 0)
    value_heads = scatter_about(key_list[2], (TOKENS_A, KV_HEADS * HEAD_DIM), 1.0, 6.0, ((0, 8), (1, 4)))
    sink_logits = jnp.clip(1.0 + 4.0 * jax.random.uniform(key_list[3], (HEADS,), jnp.float32) ** level_of(key_list[3], (HEADS,), ((0, 4),), -0.2, 0.2), 1.0, 5.0)
    mix_weight = scatter_about(key_list[4], (HEADS * HEAD_DIM, D), (HEADS * HEAD_DIM // 64) ** -0.5, 1.0)
    expert_input = scatter_about(key_list[5], (TOKENS_B, D), 1.0, 6.0, ((0, 32),))
    norm_gain = jnp.clip(1.0 + 0.18 * jax.random.normal(key_list[6], (D,), jnp.float32), 0.1, 1.9)
    routes_keys = jax.random.split(jax.random.fold_in(key_list[7], 1), TOKENS_B // TOK_B)
    routes_turns = jax.random.permutation(jax.random.fold_in(key_list[7], 3), TOKENS_B // TOK_B)
    routes = jax.vmap(lambda own, number: routed_block(jax.random.fold_in(key_list[7], 2), own, number, TOK_B, EXPERTS, TOPK, CAP, 2))(routes_keys, routes_turns).reshape((TOKENS_B, TOPK))
    route_weights = jnp.clip(jnp.exp(math.log(1.0) - 2.3025851 * jax.random.uniform(key_list[8], (TOKENS_B, TOPK), jnp.float32) ** level_of(key_list[8], (TOKENS_B, TOPK), ((0, 32),), -0.2, 0.2)), 0.1, 1.0)
    gate_weight = scatter_about(key_list[9], (EXPERTS, D, FF), (D // 9) ** -0.5, 0.375, ((0, 32),))
    up_weight = scatter_about(key_list[10], (EXPERTS, D, FF), (D // 9) ** -0.5, 0.375, ((0, 32),))
    down_weight = scatter_about(key_list[11], (EXPERTS, FF, D), (FF * 16) ** -0.5, 0.046875, ((0, 32),))
    return {"queries": queries, "key_heads": key_heads, "value_heads": value_heads, "sink_logits": sink_logits, "mix_weight": mix_weight, "expert_input": expert_input, "norm_gain": norm_gain, "routes": routes, "route_weights": route_weights, "gate_weight": gate_weight, "up_weight": up_weight, "down_weight": down_weight}


ROPE_BASE = 10000.0
CLAMP_LIMIT = 7.0
GATE_SLOPE = 1.702
NORM_EPS = 1e-05

def rotate_pairs(table, grid_rows, grid_cols, head_width):
    length = table.shape[0]
    quarter = head_width // 4
    shaped = table.reshape(length, -1, 2, 2, quarter)
    freqs = ROPE_BASE ** (-jnp.arange(0, head_width // 2, 2, dtype=jnp.float32) / (head_width // 2))
    angles = jnp.stack([grid_rows, grid_cols], axis=-1)[:, :, None] * freqs
    cosines = jnp.cos(angles)[:, None]
    sine_part = jnp.sin(angles)[:, None]
    former = shaped[..., 0, :]
    latter = shaped[..., 1, :]
    turned = jnp.stack([former * cosines - latter * sine_part, latter * cosines + former * sine_part], axis=-2)
    return turned.reshape(length, -1)

def grid_place(positions):
    return ((positions // GRID_W).astype(jnp.float32), (positions % GRID_W).astype(jnp.float32))

def attend(queries, key_heads, value_heads, sink_logits):
    length = queries.shape[0]
    group_size = HEADS // KV_HEADS
    positions = jnp.arange(length, dtype=jnp.int32)
    grid_rows, grid_cols = grid_place(positions)
    q_rot = rotate_pairs(queries.astype(jnp.float32), grid_rows, grid_cols, HEAD_DIM).astype(jnp.bfloat16)
    k_rot = rotate_pairs(key_heads.astype(jnp.float32), grid_rows, grid_cols, HEAD_DIM).astype(jnp.bfloat16)
    k_padded = jnp.pad(k_rot, ((WINDOW, WINDOW), (0, 0)))
    v_padded = jnp.pad(value_heads, ((WINDOW, WINDOW), (0, 0)))
    block_rows = math.gcd(length, 512)
    key_span = block_rows + 2 * WINDOW
    sink_grid = sink_logits.astype(jnp.float32).reshape(KV_HEADS, group_size)

    def one_block(block_index):
        first_row = block_index * block_rows
        q_blk = lax.dynamic_slice_in_dim(q_rot, first_row, block_rows, 0).astype(jnp.float32)
        q_blk = q_blk.reshape(block_rows, KV_HEADS, group_size, HEAD_DIM)
        k_blk = lax.dynamic_slice_in_dim(k_padded, first_row, key_span, 0).astype(jnp.float32)
        k_blk = k_blk.reshape(key_span, KV_HEADS, HEAD_DIM)
        v_blk = lax.dynamic_slice_in_dim(v_padded, first_row, key_span, 0).astype(jnp.float32)
        v_blk = v_blk.reshape(key_span, KV_HEADS, HEAD_DIM)
        q_pos = first_row + jnp.arange(block_rows, dtype=jnp.int32)
        k_pos = first_row - WINDOW + jnp.arange(key_span, dtype=jnp.int32)
        inside = (jnp.abs(q_pos[:, None] - k_pos[None, :]) <= WINDOW) & (k_pos >= 0) & (k_pos < length)
        scores = jnp.einsum('qkgd,skd->kgqs', q_blk, k_blk) * HEAD_DIM ** (-0.5)
        scores = jnp.where(inside, scores, -jnp.inf)
        peak = jnp.maximum(lax.optimization_barrier(jnp.max(scores, axis=-1)), sink_grid[:, :, None])
        weights_exp = jnp.exp(scores - peak[..., None])
        denominator = lax.optimization_barrier(jnp.sum(weights_exp, axis=-1)) + jnp.exp(sink_grid[:, :, None] - peak)
        chances = (weights_exp / denominator[..., None]).astype(jnp.bfloat16)
        blended = jnp.einsum('kgqs,skd->qkgd', chances.astype(jnp.float32), v_blk)
        return blended.astype(jnp.bfloat16).reshape(block_rows, HEADS * HEAD_DIM)
    blocks = lax.map(one_block, jnp.arange(length // block_rows, dtype=jnp.int32))
    return blocks.reshape(length, HEADS * HEAD_DIM)

def normalize(tokens_in, gain_row):
    values = tokens_in.astype(jnp.float32)
    center = lax.optimization_barrier(jnp.mean(values, axis=-1, keepdims=True))
    spread = lax.optimization_barrier(jnp.mean(jnp.square(values - center), axis=-1, keepdims=True))
    return ((values - center) * lax.rsqrt(spread + NORM_EPS) * gain_row.astype(jnp.float32)).astype(jnp.bfloat16)

def expert_rows(row_block, w_gate, w_lift, w_down):
    gate_pre = jnp.dot(row_block, w_gate, preferred_element_type=jnp.float32)
    lift_pre = jnp.dot(row_block, w_lift, preferred_element_type=jnp.float32)
    gate_pre = jnp.minimum(gate_pre, CLAMP_LIMIT)
    lift_pre = jnp.clip(lift_pre, -CLAMP_LIMIT, CLAMP_LIMIT)
    activated = ((lift_pre + 1.0) * gate_pre * jax.nn.sigmoid(GATE_SLOPE * gate_pre)).astype(jnp.bfloat16)
    return jnp.dot(activated, w_down, preferred_element_type=jnp.float32).astype(jnp.bfloat16)

def slot_within(route_block):
    flat_routes = route_block.reshape(-1)
    matches = (flat_routes[:, None] == jnp.arange(EXPERTS, dtype=jnp.int32)[None, :]).astype(jnp.int32)
    earlier = jnp.cumsum(matches, axis=0) - matches
    return lax.optimization_barrier(jnp.sum(earlier * matches, axis=1)).astype(jnp.int32)

def reference(queries, key_heads, value_heads, sink_logits, mix_weight, expert_input, norm_gain, routes, route_weights, gate_weight, up_weight, down_weight):
    attended = attend(queries, key_heads, value_heads, sink_logits)
    mixer_out = jnp.dot(attended, mix_weight, preferred_element_type=jnp.float32).astype(jnp.bfloat16)
    sources = N_EP * N_TP
    normed = normalize(expert_input, norm_gain)
    slots = jax.vmap(slot_within)(routes.reshape(sources, TOK_B, TOPK)).reshape(-1)
    flat_routes = routes.reshape(-1).astype(jnp.int32)
    token_of = (jnp.arange(TOKENS_B * TOPK, dtype=jnp.int32) // TOPK).astype(jnp.int32)
    source_of = (token_of // TOK_B).astype(jnp.int32)
    columns = (source_of * CAP + slots).astype(jnp.int32)
    table = jnp.full((EXPERTS, sources * CAP), TOKENS_B, jnp.int32).at[flat_routes, columns].set(token_of)
    padded_in = jnp.concatenate([normed, jnp.zeros((1, D), jnp.bfloat16)], axis=0)

    def one_expert(bundle):
        row_ids, w_gate, w_lift, w_down = bundle
        return expert_rows(padded_in[row_ids], w_gate, w_lift, w_down)
    results = lax.map(one_expert, (table, gate_weight, up_weight, down_weight))
    picked = results[flat_routes, columns].reshape(TOKENS_B, TOPK, D)
    summed = lax.optimization_barrier(jnp.sum(route_weights.astype(jnp.float32)[..., None] * picked.astype(jnp.float32), axis=1))
    return (mixer_out, summed.astype(jnp.bfloat16))
```

```python
import functools

import jax
import jax.numpy as jnp
import numpy as np
from jax import lax
from jax.experimental import pallas as pl
from jax.experimental.pallas import tpu as pltpu
from jax.sharding import Mesh
from jax.sharding import PartitionSpec as P

HEAD_DIM = 64
WINDOW = 128
GRID_W = 64
ROPE_BASE = 10000.0
CLAMP_LIMIT = 7.0
GATE_SLOPE = 1.702
NORM_EPS = 1e-05

F32 = jnp.float32
BF16 = jnp.bfloat16
MESH = pl.DeviceIdType.MESH
PANELS = 2
TILE = 256

scope = jax.named_scope


def table_rows(rows_here):
    return -(-(rows_here + 2 * WINDOW) // GRID_W // 8) * 8


def angle_tables(length, rows_here):
    half = HEAD_DIM // 2
    quarter = HEAD_DIM // 4
    lane = np.arange(2 * HEAD_DIM) % HEAD_DIM
    freqs = (ROPE_BASE ** (-np.arange(0, half, 2) / half)).astype(np.float32)
    lane_freq = np.tile(freqs, 2 * HEAD_DIM // quarter)
    count = (length - rows_here) // GRID_W + table_rows(rows_here)
    by_row = np.arange(count) - WINDOW // GRID_W
    by_col = np.arange(WINDOW) % GRID_W
    place = np.concatenate([by_row, by_col]).astype(np.float32)
    angle = (place[:, None] * lane_freq[None, :]).astype(np.float64)
    sign = np.where(lane % half < quarter, -1.0, 1.0)
    return np.stack([np.cos(angle), np.sin(angle) * sign]).astype(np.float32)


def turn(cells, cosines, sines):
    quarter = HEAD_DIM // 4
    width = cells.shape[1]
    lane = lax.broadcasted_iota(jnp.int32, cells.shape, 1)
    ahead = pltpu.roll(cells, width - quarter, 1)
    behind = pltpu.roll(cells, quarter, 1)
    partner = jnp.where(lane % (2 * quarter) < quarter, ahead, behind)
    return cells * cosines + partner * sines

def kernel(
    sizes,
    sink_hbm,
    route_hbm,
    share_hbm,
    x_hbm,
    gain_hbm,
    q_hbm,
    k_hbm,
    v_hbm,
    table_hbm,
    wg_hbm,
    wu_hbm,
    wd_hbm,
    mix_hbm,
    mixer_hbm,
    expert_hbm,
    sink,
    route_ref,
    share_ref,
    x_ref,
    gain_ref,
    q_ref,
    k_ref,
    v_ref,
    by_row,
    by_col,
    mixer_ref,
    expert_ref,
    k_scr,
    v_scr,
    halo,
    att,
    att_in,
    routing,
    normed,
    picks,
    outgoing,
    arrived,
    produced,
    returned,
    shares,
    partial,
    home,
    wg,
    wu,
    wd,
    mix,
    act,
    z_send,
    z_recv,
    rt_send,
    rt_recv,
    out_send,
    out_recv,
    back_send,
    back_recv,
    home_send,
    home_recv,
    att_send,
    att_recv,
    halo_send,
    halo_recv,
    load_sem,
):
    n_z, n_x, n_tp, top_count, capacity = sizes
    n_ep = n_z * n_x
    plane = n_x * n_tp
    slots = plane * capacity
    z, x, t = lax.axis_index("zz"), lax.axis_index("xx"), lax.axis_index("tp")
    me = x * n_tp + t
    ep = z * n_x + x
    rows_here, width_q = q_ref.shape
    tok, width = x_ref.shape
    panel = width // PANELS
    length = rows_here * n_ep
    kv_local = k_scr.shape[0]
    bq = WINDOW
    span = bq + 2 * WINDOW
    blocks = rows_here // bq
    chunk = rows_here // n_tp
    last = n_z - 1
    grid_rows = by_row.shape[1]
    table_end = table_hbm.shape[1] - WINDOW

    def z_dev(b):
        return (b, x, t)

    def plane_dev(p):
        return (z, lax.div(p, n_tp), lax.rem(p, n_tp))

    def ep_dev(e):
        return (lax.div(e, n_x), lax.rem(e, n_x), t)

    after, before = lax.rem(ep + 1, n_ep), lax.rem(ep + n_ep - 1, n_ep)
    has_after, has_before = ep < n_ep - 1, ep > 0
    has_up, has_down = z < last, z > 0
    end = (z == 0) | (z == last)
    mid = (z > 0) & (z < last)

    closer = jnp.minimum(z, last - z)
    far_side = jnp.where(z < last - z, 1, -1)

    def nearest(i):
        if i == 0:
            return z
        paired = z + ((i + 1) // 2) * (-1 if i % 2 else 1)
        return jnp.where(i <= 2 * closer, paired, z + far_side * (i - closer))

    def going_back(i):
        return lax.bitwise_xor(z, jnp.int32(last - i))

    first_row = pl.multiple_of(ep * (rows_here // GRID_W), 8)
    loads = {
        "x": (x_hbm, x_ref),
        "gain": (gain_hbm, gain_ref),
        "route": (route_hbm, route_ref),
        "share": (share_hbm, share_ref),
        "sink": (sink_hbm, sink),
        "k": (k_hbm, k_ref),
        "v": (v_hbm, v_ref),
        "by_row": (table_hbm.at[:, pl.ds(first_row, grid_rows)], by_row),
        "by_col": (table_hbm.at[:, pl.ds(table_end, WINDOW)], by_col),
        "q": (q_hbm, q_ref),
        "wg": (wg_hbm.at[0], wg),
        "wu": (wu_hbm.at[0], wu),
        "wd": (wd_hbm.at[0], wd),
        "mix": (mix_hbm, mix),
    }
    loads = {
        name: pltpu.make_async_copy(source, target, load_sem.at[i])
        for i, (name, (source, target)) in enumerate(loads.items())
    }
    for load in loads.values():
        load.start()

    def loaded(*names):
        for name in names:
            loads[name].wait()

    barrier = pltpu.get_barrier_semaphore()

    def greet_z(o, _):
        pl.semaphore_signal(barrier, inc=1, device_id=z_dev(lax.rem(z + o, n_z)), device_id_type=MESH)
        return 0

    def greet_plane(p, _):
        pl.semaphore_signal(
            barrier, inc=1, device_id=plane_dev(lax.rem(me + p, plane)), device_id_type=MESH
        )
        return 0

    lax.fori_loop(1, n_z, greet_z, 0)
    lax.fori_loop(1, plane, greet_plane, 0)
    for e in (after, before):
        pl.semaphore_signal(barrier, inc=1, device_id=ep_dev(e), device_id_type=MESH)

    loaded("x", "gain")
    with scope("norm"):
        for part in range(tok // 32):
            rows = slice(part * 32, part * 32 + 32)
            values = x_ref[rows, :].astype(F32)
            center = jnp.mean(values, axis=1, keepdims=True)
            spread = jnp.mean(jnp.square(values - center), axis=1, keepdims=True)
            result = ((values - center) * lax.rsqrt(spread + NORM_EPS) * gain_ref[...]).astype(BF16)
            for h in range(PANELS):
                normed[z, h, rows, :] = result[:, h * panel : h * panel + panel]
    loaded("route", "share")
    routing[z, :top_count, :] = route_ref[...].astype(F32)
    routing[z, top_count:, :] = share_ref[...]
    with scope("barr"):
        pl.semaphore_wait(barrier, n_z - 1 + plane - 1 + 2)

    def rt_copy(o):
        return pltpu.make_async_remote_copy(
            src_ref=routing.at[z],
            dst_ref=routing.at[z],
            send_sem=rt_send.at[o],
            recv_sem=rt_recv.at[z],
            device_id=z_dev(lax.rem(z + o, n_z)),
            device_id_type=MESH,
        )

    def z_copy(i, h, b, target):
        return pltpu.make_async_remote_copy(
            src_ref=normed.at[b, h],
            dst_ref=normed.at[b, h],
            send_sem=z_send.at[i, h],
            recv_sem=z_recv.at[b, h],
            device_id=z_dev(target),
            device_id_type=MESH,
        )

    def onward(i):
        b = nearest(i)
        target = jnp.where(b < z, z + 1, z - 1)
        return b, target, (target >= 0) & (target <= last)

    for o in range(1, n_z):
        rt_copy(o).start()
    if n_z > 1:
        for h in range(PANELS):

            @pl.when(has_up)
            def _():
                z_copy(0, h, z, z + 1).start()

            @pl.when(has_down)
            def _():
                z_copy(n_z, h, z, z - 1).start()

    def await_bytes(ref, sem):
        pltpu.make_async_copy(ref, ref, sem).wait()

    def tick(distance, h):
        for i in range(1, n_z):
            if not (i + 1) // 2 <= distance <= i:
                continue
            b, target, goes_on = onward(i)

            @pl.when(jnp.abs(b - z) == distance)
            def _():
                with scope(f"zwait{i}{h}"):
                    await_bytes(normed.at[b, h], z_recv.at[b, h])

                @pl.when(goes_on)
                def _():
                    z_copy(i, h, b, target).start()

    slot_row = lax.broadcasted_iota(jnp.int32, (slots, tok), 0)

    def choose(i):
        b = nearest(i)
        if i > 0:
            await_bytes(routing.at[b], rt_recv.at[b])
        lane_expert = (z * plane + lax.div(slot_row, capacity)).astype(F32)
        place_in = lax.rem(slot_row, capacity).astype(F32)
        upper = (
            lax.broadcasted_iota(jnp.int32, (tok, tok), 0) < lax.broadcasted_iota(jnp.int32, (tok, tok), 1)
        ).astype(F32).astype(BF16)
        route = routing[b]
        member = jnp.zeros((slots, tok), F32)
        share = jnp.zeros((slots, tok), F32)
        for k in range(top_count):
            hit = route[k : k + 1, :] == lane_expert
            member = jnp.where(hit, 1.0, member)
            share = jnp.where(hit, route[top_count + k : top_count + k + 1, :], share)
        rank = jnp.dot(member.astype(BF16), upper, preferred_element_type=F32)
        pick = jnp.where(rank == place_in, member, 0.0)
        picks[...] = pick.astype(BF16)
        scaled = (share * pick).T
        coarse = scaled.astype(BF16)
        shares[b, 0] = coarse
        shares[b, 1] = (scaled - coarse.astype(F32)).astype(BF16)

    def dispatch(i, h):
        b = nearest(i)
        with scope(f"disp{i}{h}"):
            if h == 0:
                choose(i)

            def tile(j, _):
                cols = pl.ds(pl.multiple_of(j * TILE, TILE), TILE)
                outgoing[b, h, :, cols] = jnp.dot(
                    picks[...], normed[b, h, :, cols], preferred_element_type=F32
                ).astype(BF16)
                return 0

            lax.fori_loop(0, panel // TILE, tile, 0)
            exchange(outgoing, arrived, out_send, out_recv, b, h)

    def exchange(source, target, send, recv, b, h):
        mine = pl.ds(pl.multiple_of(me * capacity, capacity), capacity)

        def one(p, _):
            to = lax.rem(me + p, plane)
            pltpu.make_async_remote_copy(
                src_ref=source.at[b, h, pl.ds(pl.multiple_of(to * capacity, capacity), capacity)],
                dst_ref=target.at[b, h, mine],
                send_sem=send.at[b, h],
                recv_sem=recv.at[b, h],
                device_id=plane_dev(to),
                device_id_type=MESH,
            ).start()
            return 0

        lax.fori_loop(1, plane, one, 0)
        pltpu.make_async_copy(source.at[b, h, mine], target.at[b, h, mine], recv.at[b, h]).start()

    def halo_copy(source, which, start, target):
        return pltpu.make_async_remote_copy(
            src_ref=source.at[pl.ds(start, WINDOW)],
            dst_ref=halo.at[which],
            send_sem=halo_send.at[which],
            recv_sem=halo_recv.at[which],
            device_id=ep_dev(target),
            device_id_type=MESH,
        )

    to_after = [
        halo_copy(k_ref, 0, rows_here - WINDOW, after),
        halo_copy(v_ref, 1, rows_here - WINDOW, after),
    ]
    to_before = [halo_copy(k_ref, 2, 0, before), halo_copy(v_ref, 3, 0, before)]

    def send_halos():
        for there, copies in ((has_after, to_after), (has_before, to_before)):

            @pl.when(there)
            def _():
                for copy in copies:
                    copy.start()

    def await_halos():
        for there, copies in ((has_before, to_after), (has_after, to_before)):

            @pl.when(there)
            def _():
                for copy in copies:
                    copy.wait_recv()

        for there, which in ((has_before, 0), (has_after, 2)):

            @pl.when(jnp.logical_not(there))
            def _():
                halo[which] = jnp.zeros(halo.shape[1:], BF16)
                halo[which + 1] = jnp.zeros(halo.shape[1:], BF16)

    of_row = lax.rem(lax.broadcasted_iota(jnp.int32, (WINDOW, 128), 1), HEAD_DIM) < HEAD_DIM // 2

    def angles(which, at):
        start = lax.div(at, GRID_W)
        parts = [
            jnp.broadcast_to(by_row[which, pl.ds(start + i, 1), :], (GRID_W, 128))
            for i in range(WINDOW // GRID_W)
        ]
        return jnp.where(of_row, jnp.concatenate(parts, axis=0), by_col[which])

    def place(source, values, at, count):
        cosines, sines = angles(0, at), angles(1, at)
        for pair in range(kv_local // 2):
            cols = slice(pair * 128, pair * 128 + 128)
            turned = turn(source[:, cols].astype(F32), cosines, sines).astype(BF16)
            piece = values[:, cols]
            for side in range(2):
                lanes = slice(side * 64, side * 64 + 64)
                k_scr[2 * pair + side, pl.ds(at, count), :] = turned[:, lanes]
                v_scr[2 * pair + side, pl.ds(at, count), :] = piece[:, lanes]

    def place_own(i, _):
        at = pl.multiple_of(i * 128, 128)
        place(k_ref[pl.ds(at, 128), :], v_ref[pl.ds(at, 128), :], WINDOW + at, 128)
        return 0

    row = lax.rem(lax.broadcasted_iota(jnp.int32, (2 * bq, span), 0), bq)
    col = lax.broadcasted_iota(jnp.int32, (2 * bq, span), 1)
    top = lax.broadcasted_iota(jnp.int32, (2 * bq, 1), 0) < bq

    def attend(block, _):
        first = pl.multiple_of(block * bq, bq)
        cosines = angles(0, first + WINDOW) * HEAD_DIM**-0.5
        sines = angles(1, first + WINDOW) * HEAD_DIM**-0.5
        key_pos = ep * rows_here + first - WINDOW + col
        inside = (col >= row) & (col <= row + 2 * WINDOW) & (key_pos >= 0) & (key_pos < length)
        for g in range(kv_local):
            q = q_ref[pl.ds(first, bq), g * 128 : g * 128 + 128].astype(F32)
            q = turn(q, cosines, sines).astype(BF16)
            q2 = jnp.concatenate([q[:, :64], q[:, 64:]], axis=0)
            k = k_scr[g, pl.ds(first, span), :]
            v = v_scr[g, pl.ds(first, span), :]
            scores = lax.dot_general(q2, k, (((1,), (1,)), ((), ())), preferred_element_type=F32)
            scores = jnp.where(inside, scores, -jnp.inf)
            logit = jnp.where(top, sink[2 * g], sink[2 * g + 1])
            peak = jnp.maximum(jnp.max(scores, axis=1, keepdims=True), logit)
            weights = jnp.exp(scores - peak)
            total = jnp.sum(weights, axis=1, keepdims=True) + jnp.exp(logit - peak)
            chances = (weights * (1.0 / total)).astype(BF16)
            blend = jnp.dot(chances, v, preferred_element_type=F32).astype(BF16)
            att[pl.ds(first, bq), g * 128 : g * 128 + 128] = jnp.concatenate(
                [blend[:bq], blend[bq:]], axis=1
            )
        return 0

    def attend_inner(part, parts):
        inner = blocks - 2
        with scope(f"att{part}"):
            lax.fori_loop(1 + inner * part // parts, 1 + inner * (part + 1) // parts, attend, 0)

    def attend_edges():
        with scope("halowait"):
            await_halos()
        with scope("edges"):
            place(halo[0], halo[1], 0, WINDOW)
            place(halo[2], halo[3], WINDOW + rows_here, WINDOW)
            lax.fori_loop(0, 2, lambda i, _: attend(i * (blocks - 1), _), 0)

    def send_heads():
        def one(p, _):
            to = lax.rem(t + p, n_tp)
            pltpu.make_async_remote_copy(
                src_ref=att.at[pl.ds(pl.multiple_of(to * chunk, chunk), chunk)],
                dst_ref=att_in.at[t],
                send_sem=att_send,
                recv_sem=att_recv,
                device_id=(z, x, to),
                device_id_type=MESH,
            ).start()
            return 0

        lax.fori_loop(1, n_tp, one, 0)
        own = pl.ds(pl.multiple_of(t * chunk, chunk), chunk)
        pltpu.make_async_copy(att.at[own], att_in.at[t], att_recv).start()

    mixer_out = pltpu.make_async_copy(mixer_ref, mixer_hbm, load_sem.at[len(loads)])

    def mixer():
        with scope("attwait"):
            await_bytes(att_in, att_recv)
        loaded("mix")

        def tile(j, _):
            cols = pl.ds(pl.multiple_of(j * TILE, TILE), TILE)
            total = jnp.zeros((chunk, TILE), F32)
            for s in range(n_tp):
                total = total + jnp.dot(
                    att_in[s], mix[s * width_q : s * width_q + width_q, cols], preferred_element_type=F32
                )
            mixer_ref[:, cols] = total.astype(BF16)
            return 0

        with scope("mixer"):
            lax.fori_loop(0, width // TILE, tile, 0)
        mixer_out.start()

    def experts(i, sent=lambda h: None):
        b = nearest(i)
        hidden = wg.shape[1]
        for h in range(PANELS):
            with scope(f"arrwait{i}{h}"):
                await_bytes(arrived.at[b, h], out_recv.at[b, h])

        def up(j, _):
            cols = pl.ds(pl.multiple_of(j * TILE, TILE), TILE)
            gate = jnp.zeros((slots, TILE), F32)
            lift = jnp.zeros((slots, TILE), F32)
            for h in range(PANELS):
                rows = arrived[b, h]
                deep = slice(h * panel, h * panel + panel)
                gate = gate + jnp.dot(rows, wg[deep, cols], preferred_element_type=F32)
                lift = lift + jnp.dot(rows, wu[deep, cols], preferred_element_type=F32)
            gate = jnp.minimum(gate, CLAMP_LIMIT)
            lift = jnp.clip(lift, -CLAMP_LIMIT, CLAMP_LIMIT)
            act[:, cols] = ((lift + 1.0) * gate * jax.nn.sigmoid(GATE_SLOPE * gate)).astype(BF16)
            return 0

        with scope(f"exp{i}"):
            lax.fori_loop(0, hidden // TILE, up, 0)
            for h in range(PANELS):

                def down(j, _):
                    cols = pl.ds(pl.multiple_of(j * TILE, TILE), TILE)
                    wide = pl.ds(pl.multiple_of(h * panel + j * TILE, TILE), TILE)
                    produced[b, h, :, cols] = jnp.dot(
                        act[...], wd[:, wide], preferred_element_type=F32
                    ).astype(BF16)
                    return 0

                lax.fori_loop(0, panel // TILE, down, 0)
                sent(h)

    def send_back(b, h):
        exchange(produced, returned, back_send, back_recv, b, h)

    def home_copy(b, h):
        target = jnp.where(b < z, z - 1, z + 1)
        slot = jnp.where((target == b) & (b < z), n_z, b)
        return pltpu.make_async_remote_copy(
            src_ref=partial.at[b, h],
            dst_ref=home.at[slot, h],
            send_sem=home_send.at[b, h],
            recv_sem=home_recv.at[slot, h],
            device_id=z_dev(target),
            device_id_type=MESH,
        )

    def clear_home():
        for slot in range(n_z + 1):
            from_up = (slot < z) | (slot == n_z)
            missing = jnp.where(from_up, z == last, z == 0)

            @pl.when(missing)
            def _():
                home[slot] = jnp.zeros(home.shape[1:], BF16)

    def weighted(b, h, cols):
        rows = returned[b, h, :, cols]
        total = jnp.dot(shares[b, 0], rows, preferred_element_type=F32)
        return total + jnp.dot(shares[b, 1], rows, preferred_element_type=F32)

    def combine(name, b, h):
        with scope(f"retwait{name}{h}"):
            await_bytes(returned.at[b, h], back_recv.at[b, h])

        @pl.when(mid)
        def _():
            with scope(f"chain{name}{h}"):
                await_bytes(home.at[b, h], home_recv.at[b, h])

        def tile(j, _):
            cols = pl.ds(pl.multiple_of(j * TILE, TILE), TILE)
            total = weighted(b, h, cols) + home[b, h, :, cols].astype(F32)
            partial[b, h, :, cols] = total.astype(BF16)
            return 0

        with scope(f"comb{name}{h}"):
            lax.fori_loop(0, panel // TILE, tile, 0)
        home_copy(b, h).start()

    expert_out = [
        pltpu.make_async_copy(
            expert_ref.at[:, pl.ds(h * panel, panel)],
            expert_hbm.at[:, pl.ds(h * panel, panel)],
            load_sem.at[len(loads) + 1 + h],
        )
        for h in range(PANELS)
    ]

    def combine_own(h):
        with scope(f"retwaitown{h}"):
            await_bytes(returned.at[z, h], back_recv.at[z, h])

        with scope(f"homewait{h}"):

            @pl.when(has_down)
            def _():
                await_bytes(home.at[z, h], home_recv.at[z, h])

            @pl.when(has_up)
            def _():
                await_bytes(home.at[n_z, h], home_recv.at[n_z, h])

        def tile(j, _):
            cols = pl.ds(pl.multiple_of(j * TILE, TILE), TILE)
            wide = pl.ds(pl.multiple_of(h * panel + j * TILE, TILE), TILE)
            total = weighted(z, h, cols) + home[z, h, :, cols].astype(F32)
            total = total + home[n_z, h, :, cols].astype(F32)
            expert_ref[:, wide] = total.astype(BF16)
            return 0

        with scope(f"combown{h}"):
            lax.fori_loop(0, panel // TILE, tile, 0)
        expert_out[h].start()

    for h in range(PANELS):
        dispatch(0, h)
    clear_home()
    loaded("k", "v", "by_row", "by_col", "q", "sink")
    with scope("place"):
        lax.fori_loop(0, rows_here // 128, place_own, 0)
    attend_inner(0, 3)
    for h in range(PANELS):
        if n_z > 1:
            tick(1, h)
            dispatch(1, h)
        attend_inner(1 + h, 3)
    if n_z > 2:
        tick(2, 0)
        dispatch(2, 0)
    loaded("wg", "wu", "wd")
    if n_z == 1:
        send_halos()
    if n_z > 1:
        experts(0)
    if n_z > 2:
        tick(2, 1)
        dispatch(2, 1)
    if n_z > 1:
        send_halos()
    if n_z > 2:
        experts(1)
        for h in range(PANELS):
            tick(3, h)
            dispatch(3, h)
        experts(2)
    attend_edges()
    send_heads()
    if n_z > 2:

        @pl.when(mid)
        def _():
            for h in range(PANELS):
                send_back(going_back(0), h)

    def sent(h):
        @pl.when(end)
        def _():
            send_back(going_back(0), h)

    experts(last, sent)
    for i in range(1, n_z):
        for h in range(PANELS):
            send_back(going_back(i), h)
    mixer()
    for i in range(last):
        b = going_back(i)
        if n_z > 2:
            b = jnp.where(mid, going_back((i + 1) % last), b)
        for h in range(PANELS):
            combine(i, b, h)
    for h in range(PANELS):
        combine_own(h)

    for o in range(1, n_z):
        rt_copy(o).wait_send()
    if n_z > 1:
        for h in range(PANELS):

            @pl.when(has_up)
            def _():
                z_copy(0, h, z, z + 1).wait_send()

            @pl.when(has_down)
            def _():
                z_copy(n_z, h, z, z - 1).wait_send()

            for i in range(1, n_z):
                b, target, goes_on = onward(i)

                @pl.when(goes_on)
                def _():
                    z_copy(i, h, b, target).wait_send()

                home_copy(b, h).wait_send()
    for there, copies in ((has_after, to_after), (has_before, to_before)):

        @pl.when(there)
        def _():
            for copy in copies:
                copy.wait_send()

    for b in range(n_z):
        for h in range(PANELS):
            gone = pl.ds(0, (plane - 1) * capacity)
            await_bytes(outgoing.at[b, h, gone], out_send.at[b, h])
            await_bytes(produced.at[b, h, gone], back_send.at[b, h])
    await_bytes(att.at[pl.ds(0, (n_tp - 1) * chunk)], att_send)
    mixer_out.wait()
    for copy in expert_out:
        copy.wait()


def hand_over(mixer_in, expert_in, mixer_out, expert_out, mixer_scr, expert_scr, sem):
    steps = []
    for source, scratch, target, at, parts in (
        (mixer_in, mixer_scr, mixer_out, 0, 4),
        (expert_in, expert_scr, expert_out, 4, 2),
    ):
        rows = source.shape[0] // parts
        for part in range(parts):
            here = pl.ds(part * rows, rows)
            steps.append(
                (
                    pltpu.make_async_copy(source.at[here], scratch.at[here], sem.at[0, at + part]),
                    pltpu.make_async_copy(scratch.at[here], target.at[here], sem.at[1, at + part]),
                )
            )
    for take, _ in steps:
        take.start()
    for take, give in steps:
        take.wait()
        give.start()
    for _, give in steps:
        give.wait()


def body(
    queries,
    key_heads,
    value_heads,
    sink_logits,
    mix_weight,
    expert_input,
    norm_gain,
    routes,
    route_weights,
    gate_weight,
    up_weight,
    down_weight,
):
    n_z, n_x, n_tp = lax.axis_size("zz"), lax.axis_size("xx"), lax.axis_size("tp")
    n_ep = n_z * n_x
    plane = n_x * n_tp
    rows_here, width_q = queries.shape
    kv_width = key_heads.shape[1]
    kv_local = kv_width // HEAD_DIM
    tok, top_count = routes.shape
    capacity = 2 * tok * top_count // (n_ep * n_tp)
    slots = plane * capacity
    width = expert_input.shape[1]
    panel = width // PANELS
    hidden = gate_weight.shape[2]
    tables = jnp.asarray(angle_tables(rows_here * n_ep, rows_here))
    anywhere = pl.BlockSpec(memory_space=pl.ANY)
    reach = rows_here + 2 * WINDOW
    dma = pltpu.SemaphoreType.DMA
    shapes = [
        jax.ShapeDtypeStruct((rows_here // n_tp, width), BF16),
        jax.ShapeDtypeStruct((tok, width), BF16),
    ]
    both = dma((n_z, PANELS))
    mixed, expert = pl.pallas_call(
        functools.partial(kernel, (n_z, n_x, n_tp, top_count, capacity)),
        in_specs=[anywhere] * 13,
        out_specs=[anywhere] * 2,
        out_shape=shapes,
        scratch_shapes=[
            pltpu.SMEM(sink_logits.shape, F32),
            pltpu.VMEM((top_count, tok), jnp.int32),
            pltpu.VMEM((top_count, tok), F32),
            pltpu.VMEM((tok, width), BF16),
            pltpu.VMEM((1, width), F32),
            pltpu.VMEM((rows_here, width_q), BF16),
            pltpu.VMEM((rows_here, kv_width), BF16),
            pltpu.VMEM((rows_here, kv_width), BF16),
            pltpu.VMEM((2, table_rows(rows_here), 128), F32),
            pltpu.VMEM((2, WINDOW, 128), F32),
            pltpu.VMEM((rows_here // n_tp, width), BF16),
            pltpu.VMEM((tok, width), BF16),
            pltpu.VMEM((kv_local, reach, HEAD_DIM), BF16),
            pltpu.VMEM((kv_local, reach, HEAD_DIM), BF16),
            pltpu.VMEM((4, WINDOW, kv_width), BF16),
            pltpu.VMEM((rows_here, width_q), BF16),
            pltpu.VMEM((n_tp, rows_here // n_tp, width_q), BF16),
            pltpu.VMEM((n_z, 2 * top_count, tok), F32),
            pltpu.VMEM((n_z, PANELS, tok, panel), BF16),
            pltpu.VMEM((slots, tok), BF16),
            pltpu.VMEM((n_z, PANELS, slots, panel), BF16),
            pltpu.VMEM((n_z, PANELS, slots, panel), BF16),
            pltpu.VMEM((n_z, PANELS, slots, panel), BF16),
            pltpu.VMEM((n_z, PANELS, slots, panel), BF16),
            pltpu.VMEM((n_z, 2, tok, slots), BF16),
            pltpu.VMEM((n_z, PANELS, tok, panel), BF16),
            pltpu.VMEM((n_z + 1, PANELS, tok, panel), BF16),
            pltpu.VMEM((width, hidden), BF16),
            pltpu.VMEM((width, hidden), BF16),
            pltpu.VMEM((hidden, width), BF16),
            pltpu.VMEM(mix_weight.shape, BF16),
            pltpu.VMEM((slots, hidden), BF16),
            dma((n_z + 1, PANELS)),
            both,
            dma((n_z,)),
            dma((n_z,)),
            both,
            both,
            both,
            both,
            both,
            dma((n_z + 1, PANELS)),
            dma,
            dma,
            dma((4,)),
            dma((4,)),
            dma((15 + PANELS,)),
        ],
        compiler_params=pltpu.CompilerParams(
            collective_id=0, has_side_effects=True, vmem_limit_bytes=67043328
        ),
        name="layer",
    )(
        sink_logits,
        routes.T,
        route_weights.T,
        expert_input,
        norm_gain[None, :],
        queries,
        key_heads,
        value_heads,
        tables,
        gate_weight,
        up_weight,
        down_weight,
        mix_weight,
    )
    return pl.pallas_call(
        hand_over,
        in_specs=[anywhere] * 2,
        out_specs=[anywhere] * 2,
        out_shape=shapes,
        scratch_shapes=[pltpu.VMEM(s.shape, BF16) for s in shapes] + [dma((2, 6))],
        name="hand_over",
    )(mixed, expert)


def z_count(mesh, n_ep):
    coords = {getattr(d, "coords", (0, 0, 0))[2] for d in mesh.devices.flat}
    return len(coords) if len(coords) in (2, 4) and n_ep % len(coords) == 0 else 1


def solution(mesh):
    n_ep, n_tp = mesh.shape["ep"], mesh.shape["tp"]
    n_z = z_count(mesh, n_ep)
    grid = Mesh(mesh.devices.reshape(n_z, n_ep // n_z, n_tp), ("zz", "xx", "tp"))
    ep = ("zz", "xx")
    every = ("zz", "xx", "tp")
    return jax.shard_map(
        body,
        mesh=grid,
        in_specs=(
            P(ep, "tp"),
            P(ep, "tp"),
            P(ep, "tp"),
            P("tp"),
            P(),
            P(every, None),
            P(),
            P(every, None),
            P(every, None),
            P(every, None, None),
            P(every, None, None),
            P(every, None, None),
        ),
        out_specs=(P(every, None), P(every, None)),
        check_vma=False,
    )
```

```python
import functools

import jax
import jax.numpy as jnp
import numpy as np
from jax import lax
from jax.experimental import pallas as pl
from jax.experimental.pallas import tpu as pltpu
from jax.sharding import Mesh
from jax.sharding import PartitionSpec as P

HEAD_DIM = 64
WINDOW = 128
GRID_W = 64
ROPE_BASE = 10000.0
CLAMP_LIMIT = 7.0
GATE_SLOPE = 1.702
NORM_EPS = 1e-05

F32 = jnp.float32
BF16 = jnp.bfloat16
MESH = pl.DeviceIdType.MESH
PANELS = 2
TILE = 256
VMEM_BYTES = 61 << 20

scope = jax.named_scope


def table_rows(rows_here):
    return -(-(rows_here + 2 * WINDOW) // GRID_W // 8) * 8


def angle_tables(length, rows_here):
    half = HEAD_DIM // 2
    quarter = HEAD_DIM // 4
    lane = np.arange(2 * HEAD_DIM) % HEAD_DIM
    freqs = (ROPE_BASE ** (-np.arange(0, half, 2) / half)).astype(np.float32)
    lane_freq = np.tile(freqs, 2 * HEAD_DIM // quarter)
    count = (length - rows_here) // GRID_W + table_rows(rows_here)
    by_row = np.arange(count) - WINDOW // GRID_W
    by_col = np.arange(WINDOW) % GRID_W
    place = np.concatenate([by_row, by_col]).astype(np.float32)
    angle = (place[:, None] * lane_freq[None, :]).astype(np.float64)
    sign = np.where(lane % half < quarter, -1.0, 1.0)
    return np.stack([np.cos(angle), np.sin(angle) * sign]).astype(np.float32)


def turn(cells, cosines, sines):
    quarter = HEAD_DIM // 4
    width = cells.shape[1]
    lane = lax.broadcasted_iota(jnp.int32, cells.shape, 1)
    ahead = pltpu.roll(cells, width - quarter, 1)
    behind = pltpu.roll(cells, quarter, 1)
    partner = jnp.where(lane % (2 * quarter) < quarter, ahead, behind)
    return cells * cosines + partner * sines

def kernel(
    sizes,
    sink_hbm,
    route_hbm,
    share_hbm,
    x_hbm,
    gain_hbm,
    q_hbm,
    k_hbm,
    v_hbm,
    table_hbm,
    wg_hbm,
    wu_hbm,
    wd_hbm,
    mix_hbm,
    mixer_ref,
    expert_ref,
    sink,
    route_ref,
    share_ref,
    x_ref,
    gain_ref,
    q_ref,
    k_ref,
    v_ref,
    by_row,
    by_col,
    k_scr,
    v_scr,
    halo,
    att,
    att_in,
    routing,
    normed,
    picks,
    outgoing,
    arrived,
    produced,
    returned,
    shares,
    partial,
    home,
    wg,
    wu,
    wd,
    mix,
    act,
    z_send,
    z_recv,
    rt_send,
    rt_recv,
    out_send,
    out_recv,
    back_send,
    back_recv,
    home_send,
    home_recv,
    att_send,
    att_recv,
    halo_send,
    halo_recv,
    load_sem,
):
    n_z, n_x, n_tp, top_count, capacity = sizes
    n_ep = n_z * n_x
    plane = n_x * n_tp
    slots = plane * capacity
    z, x, t = lax.axis_index("zz"), lax.axis_index("xx"), lax.axis_index("tp")
    me = x * n_tp + t
    ep = z * n_x + x
    rows_here, width_q = q_ref.shape
    tok, width = x_ref.shape
    panel = width // PANELS
    length = rows_here * n_ep
    kv_local = k_scr.shape[0]
    bq = WINDOW
    span = bq + 2 * WINDOW
    blocks = rows_here // bq
    chunk = rows_here // n_tp
    last = n_z - 1
    grid_rows = by_row.shape[1]
    table_end = table_hbm.shape[1] - WINDOW

    def z_dev(b):
        return (b, x, t)

    def plane_dev(p):
        return (z, lax.div(p, n_tp), lax.rem(p, n_tp))

    def ep_dev(e):
        return (lax.div(e, n_x), lax.rem(e, n_x), t)

    after, before = lax.rem(ep + 1, n_ep), lax.rem(ep + n_ep - 1, n_ep)
    has_after, has_before = ep < n_ep - 1, ep > 0
    has_up, has_down = z < last, z > 0
    end = (z == 0) | (z == last)
    mid = (z > 0) & (z < last)

    closer = jnp.minimum(z, last - z)
    far_side = jnp.where(z < last - z, 1, -1)

    def nearest(i):
        if i == 0:
            return z
        paired = z + ((i + 1) // 2) * (-1 if i % 2 else 1)
        return jnp.where(i <= 2 * closer, paired, z + far_side * (i - closer))

    def going_back(i):
        return lax.bitwise_xor(z, jnp.int32(last - i))

    first_row = pl.multiple_of(ep * (rows_here // GRID_W), 8)
    loads = {
        "route": (route_hbm, route_ref),
        "share": (share_hbm, share_ref),
        "x": (x_hbm, x_ref),
        "gain": (gain_hbm, gain_ref),
        "sink": (sink_hbm, sink),
        "k": (k_hbm, k_ref),
        "v": (v_hbm, v_ref),
        "by_row": (table_hbm.at[:, pl.ds(first_row, grid_rows)], by_row),
        "by_col": (table_hbm.at[:, pl.ds(table_end, WINDOW)], by_col),
        "q": (q_hbm, q_ref),
        "wg": (wg_hbm.at[0], wg),
        "wu": (wu_hbm.at[0], wu),
        "wd": (wd_hbm.at[0], wd),
        "mix": (mix_hbm, mix),
    }
    loads = {
        name: pltpu.make_async_copy(source, target, load_sem.at[i])
        for i, (name, (source, target)) in enumerate(loads.items())
    }
    for load in loads.values():
        load.start()

    def loaded(*names):
        for name in names:
            loads[name].wait()

    barrier = pltpu.get_barrier_semaphore()

    def greet_z(o, _):
        pl.semaphore_signal(barrier, inc=1, device_id=z_dev(lax.rem(z + o, n_z)), device_id_type=MESH)
        return 0

    def greet_plane(p, _):
        pl.semaphore_signal(
            barrier, inc=1, device_id=plane_dev(lax.rem(me + p, plane)), device_id_type=MESH
        )
        return 0

    lax.fori_loop(1, n_z, greet_z, 0)
    lax.fori_loop(1, plane, greet_plane, 0)
    for e in (after, before):
        pl.semaphore_signal(barrier, inc=1, device_id=ep_dev(e), device_id_type=MESH)

    def await_bytes(ref, sem):
        pltpu.make_async_copy(ref, ref, sem).wait()

    slot_row = lax.broadcasted_iota(jnp.int32, (slots, tok), 0)

    def choose(i):
        b = nearest(i)
        if i > 0:
            await_bytes(routing.at[b], rt_recv.at[b])
        lane_expert = (z * plane + lax.div(slot_row, capacity)).astype(F32)
        place_in = lax.rem(slot_row, capacity).astype(F32)
        upper = (
            lax.broadcasted_iota(jnp.int32, (tok, tok), 0) < lax.broadcasted_iota(jnp.int32, (tok, tok), 1)
        ).astype(F32).astype(BF16)
        route = routing[b]
        member = jnp.zeros((slots, tok), F32)
        share = jnp.zeros((slots, tok), F32)
        for k in range(top_count):
            hit = route[k : k + 1, :] == lane_expert
            member = jnp.where(hit, 1.0, member)
            share = jnp.where(hit, route[top_count + k : top_count + k + 1, :], share)
        rank = jnp.dot(member.astype(BF16), upper, preferred_element_type=F32)
        pick = jnp.where(rank == place_in, member, 0.0)
        picks[...] = pick.astype(BF16)
        scaled = (share * pick).T
        coarse = scaled.astype(BF16)
        shares[b, 0] = coarse
        shares[b, 1] = (scaled - coarse.astype(F32)).astype(BF16)

    loaded("route", "share")
    routing[z, :top_count, :] = route_ref[...].astype(F32)
    routing[z, top_count:, :] = share_ref[...]
    choose(0)
    loaded("x", "gain")
    with scope("norm"):
        for part in range(tok // 32):
            rows = slice(part * 32, part * 32 + 32)
            values = x_ref[rows, :].astype(F32)
            center = jnp.mean(values, axis=1, keepdims=True)
            spread = jnp.mean(jnp.square(values - center), axis=1, keepdims=True)
            result = ((values - center) * lax.rsqrt(spread + NORM_EPS) * gain_ref[...]).astype(BF16)
            for h in range(PANELS):
                normed[z, h, rows, :] = result[:, h * panel : h * panel + panel]
    with scope("barr"):
        pl.semaphore_wait(barrier, n_z - 1 + plane - 1 + 2)

    def rt_copy(o):
        return pltpu.make_async_remote_copy(
            src_ref=routing.at[z],
            dst_ref=routing.at[z],
            send_sem=rt_send.at[o],
            recv_sem=rt_recv.at[z],
            device_id=z_dev(lax.rem(z + o, n_z)),
            device_id_type=MESH,
        )

    def z_copy(i, h, b, target):
        return pltpu.make_async_remote_copy(
            src_ref=normed.at[b, h],
            dst_ref=normed.at[b, h],
            send_sem=z_send.at[i, h],
            recv_sem=z_recv.at[b, h],
            device_id=z_dev(target),
            device_id_type=MESH,
        )

    def onward(i):
        b = nearest(i)
        target = jnp.where(b < z, z + 1, z - 1)
        return b, target, (target >= 0) & (target <= last)

    for o in range(1, n_z):
        rt_copy(o).start()
    if n_z > 1:
        for h in range(PANELS):

            @pl.when(has_up)
            def _():
                z_copy(0, h, z, z + 1).start()

            @pl.when(has_down)
            def _():
                z_copy(n_z, h, z, z - 1).start()

    def tick(distance, h):
        for i in range(1, n_z):
            if not (i + 1) // 2 <= distance <= i:
                continue
            b, target, goes_on = onward(i)

            @pl.when(jnp.abs(b - z) == distance)
            def _():
                with scope(f"zwait{i}{h}"):
                    await_bytes(normed.at[b, h], z_recv.at[b, h])

                @pl.when(goes_on)
                def _():
                    z_copy(i, h, b, target).start()

    def dispatch(i, h):
        b = nearest(i)
        with scope(f"disp{i}{h}"):
            if h == 0 and i > 0:
                choose(i)

            def tile(j, _):
                cols = pl.ds(pl.multiple_of(j * TILE, TILE), TILE)
                outgoing[b, h, :, cols] = jnp.dot(
                    picks[...], normed[b, h, :, cols], preferred_element_type=F32
                ).astype(BF16)
                return 0

            lax.fori_loop(0, panel // TILE, tile, 0)
            exchange(outgoing, arrived, out_send, out_recv, b, h)

    def exchange(source, target, send, recv, b, h):
        mine = pl.ds(pl.multiple_of(me * capacity, capacity), capacity)

        def one(p, _):
            to = lax.rem(me + p, plane)
            pltpu.make_async_remote_copy(
                src_ref=source.at[b, h, pl.ds(pl.multiple_of(to * capacity, capacity), capacity)],
                dst_ref=target.at[b, h, mine],
                send_sem=send.at[b, h],
                recv_sem=recv.at[b, h],
                device_id=plane_dev(to),
                device_id_type=MESH,
            ).start()
            return 0

        lax.fori_loop(1, plane, one, 0)
        pltpu.make_async_copy(source.at[b, h, mine], target.at[b, h, mine], recv.at[b, h]).start()

    def halo_copy(source, which, start, target):
        return pltpu.make_async_remote_copy(
            src_ref=source.at[pl.ds(start, WINDOW)],
            dst_ref=halo.at[which],
            send_sem=halo_send.at[which],
            recv_sem=halo_recv.at[which],
            device_id=ep_dev(target),
            device_id_type=MESH,
        )

    to_after = [
        halo_copy(k_ref, 0, rows_here - WINDOW, after),
        halo_copy(v_ref, 1, rows_here - WINDOW, after),
    ]
    to_before = [halo_copy(k_ref, 2, 0, before), halo_copy(v_ref, 3, 0, before)]

    def send_halos():
        for there, copies in ((has_after, to_after), (has_before, to_before)):

            @pl.when(there)
            def _():
                for copy in copies:
                    copy.start()

    def await_halos():
        for there, copies in ((has_before, to_after), (has_after, to_before)):

            @pl.when(there)
            def _():
                for copy in copies:
                    copy.wait_recv()

        for there, which in ((has_before, 0), (has_after, 2)):

            @pl.when(jnp.logical_not(there))
            def _():
                halo[which] = jnp.zeros(halo.shape[1:], BF16)
                halo[which + 1] = jnp.zeros(halo.shape[1:], BF16)

    of_row = lax.rem(lax.broadcasted_iota(jnp.int32, (WINDOW, 128), 1), HEAD_DIM) < HEAD_DIM // 2

    def angles(which, at):
        start = lax.div(at, GRID_W)
        parts = [
            jnp.broadcast_to(by_row[which, pl.ds(start + i, 1), :], (GRID_W, 128))
            for i in range(WINDOW // GRID_W)
        ]
        return jnp.where(of_row, jnp.concatenate(parts, axis=0), by_col[which])

    def place(source, values, at, count):
        cosines, sines = angles(0, at), angles(1, at)
        for pair in range(kv_local // 2):
            cols = slice(pair * 128, pair * 128 + 128)
            turned = turn(source[:, cols].astype(F32), cosines, sines).astype(BF16)
            piece = values[:, cols]
            for side in range(2):
                lanes = slice(side * 64, side * 64 + 64)
                k_scr[2 * pair + side, pl.ds(at, count), :] = turned[:, lanes]
                v_scr[2 * pair + side, pl.ds(at, count), :] = piece[:, lanes]

    def place_own(i, _):
        at = pl.multiple_of(i * 128, 128)
        place(k_ref[pl.ds(at, 128), :], v_ref[pl.ds(at, 128), :], WINDOW + at, 128)
        return 0

    row = lax.rem(lax.broadcasted_iota(jnp.int32, (2 * bq, span), 0), bq)
    col = lax.broadcasted_iota(jnp.int32, (2 * bq, span), 1)
    top = lax.broadcasted_iota(jnp.int32, (2 * bq, 1), 0) < bq

    def attend(block, _):
        first = pl.multiple_of(block * bq, bq)
        cosines = angles(0, first + WINDOW) * HEAD_DIM**-0.5
        sines = angles(1, first + WINDOW) * HEAD_DIM**-0.5
        key_pos = ep * rows_here + first - WINDOW + col
        inside = (col >= row) & (col <= row + 2 * WINDOW) & (key_pos >= 0) & (key_pos < length)
        for g in range(kv_local):
            q = q_ref[pl.ds(first, bq), g * 128 : g * 128 + 128].astype(F32)
            q = turn(q, cosines, sines).astype(BF16)
            q2 = jnp.concatenate([q[:, :64], q[:, 64:]], axis=0)
            k = k_scr[g, pl.ds(first, span), :]
            v = v_scr[g, pl.ds(first, span), :]
            scores = lax.dot_general(q2, k, (((1,), (1,)), ((), ())), preferred_element_type=F32)
            scores = jnp.where(inside, scores, -jnp.inf)
            logit = jnp.where(top, sink[2 * g], sink[2 * g + 1])
            peak = jnp.maximum(jnp.max(scores, axis=1, keepdims=True), logit)
            weights = jnp.exp(scores - peak)
            total = jnp.sum(weights, axis=1, keepdims=True) + jnp.exp(logit - peak)
            chances = (weights * (1.0 / total)).astype(BF16)
            blend = jnp.dot(chances, v, preferred_element_type=F32).astype(BF16)
            att[pl.ds(first, bq), g * 128 : g * 128 + 128] = jnp.concatenate(
                [blend[:bq], blend[bq:]], axis=1
            )
        return 0

    def attend_inner(part, parts):
        inner = blocks - 2
        with scope(f"att{part}"):
            lax.fori_loop(1 + inner * part // parts, 1 + inner * (part + 1) // parts, attend, 0)

    def attend_edges():
        with scope("halowait"):
            await_halos()
        with scope("edges"):
            place(halo[0], halo[1], 0, WINDOW)
            place(halo[2], halo[3], WINDOW + rows_here, WINDOW)
            lax.fori_loop(0, 2, lambda i, _: attend(i * (blocks - 1), _), 0)

    def send_heads(edges):
        each = chunk // bq

        def one(p, _):
            to = lax.rem(t + p, n_tp)
            for i in range(each):
                block = to * each + i
                at_edge = (block == 0) | (block == blocks - 1)

                @pl.when(at_edge if edges else jnp.logical_not(at_edge))
                def _():
                    pltpu.make_async_remote_copy(
                        src_ref=att.at[pl.ds(pl.multiple_of(block * bq, bq), bq)],
                        dst_ref=att_in.at[t, i * bq : i * bq + bq],
                        send_sem=att_send,
                        recv_sem=att_recv,
                        device_id=(z, x, to),
                        device_id_type=MESH,
                    ).start()

            return 0

        lax.fori_loop(1, n_tp, one, 0)
        if edges:
            own = pl.ds(pl.multiple_of(t * chunk, chunk), chunk)
            pltpu.make_async_copy(att.at[own], att_in.at[t], att_recv).start()

    def mixer():
        with scope("attwait"):
            await_bytes(att_in, att_recv)
        loaded("mix")

        def tile(j, _):
            cols = pl.ds(pl.multiple_of(j * TILE, TILE), TILE)
            total = jnp.zeros((chunk, TILE), F32)
            for s in range(n_tp):
                total = total + jnp.dot(
                    att_in[s], mix[s * width_q : s * width_q + width_q, cols], preferred_element_type=F32
                )
            mixer_ref[:, cols] = total.astype(BF16)
            return 0

        with scope("mixer"):
            lax.fori_loop(0, width // TILE, tile, 0)

    def experts(i, sent=lambda h: None):
        b = nearest(i)
        hidden = wg.shape[1]
        for h in range(PANELS):
            with scope(f"arrwait{i}{h}"):
                await_bytes(arrived.at[b, h], out_recv.at[b, h])

        def up(j, _):
            cols = pl.ds(pl.multiple_of(j * TILE, TILE), TILE)
            gate = jnp.zeros((slots, TILE), F32)
            lift = jnp.zeros((slots, TILE), F32)
            for h in range(PANELS):
                rows = arrived[b, h]
                deep = slice(h * panel, h * panel + panel)
                gate = gate + jnp.dot(rows, wg[deep, cols], preferred_element_type=F32)
                lift = lift + jnp.dot(rows, wu[deep, cols], preferred_element_type=F32)
            gate = jnp.minimum(gate, CLAMP_LIMIT)
            lift = jnp.clip(lift, -CLAMP_LIMIT, CLAMP_LIMIT)
            act[:, cols] = ((lift + 1.0) * gate * jax.nn.sigmoid(GATE_SLOPE * gate)).astype(BF16)
            return 0

        with scope(f"exp{i}"):
            lax.fori_loop(0, hidden // TILE, up, 0)
            for h in range(PANELS):

                def down(j, _):
                    cols = pl.ds(pl.multiple_of(j * TILE, TILE), TILE)
                    wide = pl.ds(pl.multiple_of(h * panel + j * TILE, TILE), TILE)
                    produced[b, h, :, cols] = jnp.dot(
                        act[...], wd[:, wide], preferred_element_type=F32
                    ).astype(BF16)
                    return 0

                lax.fori_loop(0, panel // TILE, down, 0)
                sent(h)

    def send_back(b, h):
        exchange(produced, returned, back_send, back_recv, b, h)

    def home_copy(b, h):
        target = jnp.where(b < z, z - 1, z + 1)
        slot = jnp.where((target == b) & (b < z), n_z, b)
        return pltpu.make_async_remote_copy(
            src_ref=partial.at[b, h],
            dst_ref=home.at[slot, h],
            send_sem=home_send.at[b, h],
            recv_sem=home_recv.at[slot, h],
            device_id=z_dev(target),
            device_id_type=MESH,
        )

    def clear_home():
        for slot in range(n_z + 1):
            from_up = (slot < z) | (slot == n_z)
            missing = jnp.where(from_up, z == last, z == 0)

            @pl.when(missing)
            def _():
                home[slot] = jnp.zeros(home.shape[1:], BF16)

    def weighted(b, h, cols):
        rows = returned[b, h, :, cols]
        total = jnp.dot(shares[b, 0], rows, preferred_element_type=F32)
        return total + jnp.dot(shares[b, 1], rows, preferred_element_type=F32)

    def combine(name, b, h):
        with scope(f"retwait{name}"):
            await_bytes(returned.at[b, h], back_recv.at[b, h])

        @pl.when(mid)
        def _():
            with scope(f"chain{name}"):
                await_bytes(home.at[b, h], home_recv.at[b, h])

        def tile(j, _):
            cols = pl.ds(pl.multiple_of(j * TILE, TILE), TILE)
            total = weighted(b, h, cols) + home[b, h, :, cols].astype(F32)
            partial[b, h, :, cols] = total.astype(BF16)
            return 0

        with scope(f"comb{name}"):
            lax.fori_loop(0, panel // TILE, tile, 0)
        home_copy(b, h).start()

    def combine_own(h):
        with scope(f"retwaitown{h}"):
            await_bytes(returned.at[z, h], back_recv.at[z, h])

        with scope(f"homewait{h}"):

            @pl.when(has_down)
            def _():
                await_bytes(home.at[z, h], home_recv.at[z, h])

            @pl.when(has_up)
            def _():
                await_bytes(home.at[n_z, h], home_recv.at[n_z, h])

        def tile(j, _):
            cols = pl.ds(pl.multiple_of(j * TILE, TILE), TILE)
            wide = pl.ds(pl.multiple_of(h * panel + j * TILE, TILE), TILE)
            total = weighted(z, h, cols) + home[z, h, :, cols].astype(F32)
            total = total + home[n_z, h, :, cols].astype(F32)
            expert_ref[:, wide] = total.astype(BF16)
            return 0

        with scope(f"combown{h}"):
            lax.fori_loop(0, panel // TILE, tile, 0)

    for h in range(PANELS):
        dispatch(0, h)
    clear_home()
    loaded("k", "v", "by_row", "by_col", "q", "sink")
    with scope("place"):
        lax.fori_loop(0, rows_here // 128, place_own, 0)
    attend_inner(0, 3)
    for h in range(PANELS):
        if n_z > 1:
            tick(1, h)
            dispatch(1, h)
        attend_inner(1 + h, 3)
    if n_z > 2:
        tick(2, 0)
        dispatch(2, 0)
    loaded("wg", "wu", "wd")
    if n_z > 1:
        experts(0)
    if n_z > 2:
        tick(2, 1)
        dispatch(2, 1)
        experts(1)
        for h in range(PANELS):
            tick(3, h)
            dispatch(3, h)
    send_halos()
    send_heads(False)
    if n_z > 2:
        experts(2)

        @pl.when(mid)
        def _():
            for h in range(PANELS):
                send_back(going_back(0), h)

    def sent(h):
        @pl.when(end)
        def _():
            send_back(going_back(0), h)

    experts(last, sent)
    attend_edges()
    send_heads(True)
    for i in range(1, n_z):
        for h in range(PANELS):
            send_back(going_back(i), h)
    order = [(i, h) for i in range(last) for h in range(PANELS)]
    if n_z > 2:
        later = [(1, h) for h in range(PANELS)] + [(i, h) for h in range(PANELS) for i in range(2, last)]
        at = len(later) - PANELS * (last - 2) + last - 2
        for h in range(PANELS):
            later.insert(at + h * (last - 1), (0, h))
    else:
        later = order
    for step, ((i, h), (j, g)) in enumerate(zip(order, later)):
        b = jnp.where(mid, going_back(j), going_back(i))
        combine(step, b, h if g == h else jnp.where(mid, g, h))
        if step == PANELS - 1:
            mixer()
    if n_z == 1:
        mixer()
    for o in range(1, n_z):
        rt_copy(o).wait_send()
    if n_z > 1:
        for h in range(PANELS):

            @pl.when(has_up)
            def _():
                z_copy(0, h, z, z + 1).wait_send()

            @pl.when(has_down)
            def _():
                z_copy(n_z, h, z, z - 1).wait_send()

            for i in range(1, n_z):
                b, target, goes_on = onward(i)

                @pl.when(goes_on)
                def _():
                    z_copy(i, h, b, target).wait_send()
    for there, copies in ((has_after, to_after), (has_before, to_before)):

        @pl.when(there)
        def _():
            for copy in copies:
                copy.wait_send()

    for b in range(n_z):
        for h in range(PANELS):
            gone = pl.ds(0, (plane - 1) * capacity)
            await_bytes(outgoing.at[b, h, gone], out_send.at[b, h])
    await_bytes(att.at[pl.ds(0, (n_tp - 1) * chunk)], att_send)

    for h in range(PANELS):
        combine_own(h)

    for h in range(PANELS):
        for i in range(1, n_z):
            home_copy(nearest(i), h).wait_send()
        for b in range(n_z):
            gone = pl.ds(0, (plane - 1) * capacity)
            await_bytes(produced.at[b, h, gone], back_send.at[b, h])


def body(
    queries,
    key_heads,
    value_heads,
    sink_logits,
    mix_weight,
    expert_input,
    norm_gain,
    routes,
    route_weights,
    gate_weight,
    up_weight,
    down_weight,
):
    n_z, n_x, n_tp = lax.axis_size("zz"), lax.axis_size("xx"), lax.axis_size("tp")
    n_ep = n_z * n_x
    plane = n_x * n_tp
    rows_here, width_q = queries.shape
    kv_width = key_heads.shape[1]
    kv_local = kv_width // HEAD_DIM
    tok, top_count = routes.shape
    capacity = 2 * tok * top_count // (n_ep * n_tp)
    slots = plane * capacity
    width = expert_input.shape[1]
    panel = width // PANELS
    hidden = gate_weight.shape[2]
    tables = jnp.asarray(angle_tables(rows_here * n_ep, rows_here))
    anywhere = pl.BlockSpec(memory_space=pl.ANY)
    vmem = pl.BlockSpec(memory_space=pltpu.VMEM)
    reach = rows_here + 2 * WINDOW
    dma = pltpu.SemaphoreType.DMA
    shapes = [
        jax.ShapeDtypeStruct((rows_here // n_tp, width), BF16),
        jax.ShapeDtypeStruct((tok, width), BF16),
    ]
    both = dma((n_z, PANELS))
    return pl.pallas_call(
        functools.partial(kernel, (n_z, n_x, n_tp, top_count, capacity)),
        in_specs=[anywhere] * 13,
        out_specs=[vmem] * 2,
        out_shape=[pltpu.VMEM(s.shape, s.dtype) for s in shapes],
        scratch_shapes=[
            pltpu.SMEM(sink_logits.shape, F32),
            pltpu.VMEM((top_count, tok), jnp.int32),
            pltpu.VMEM((top_count, tok), F32),
            pltpu.VMEM((tok, width), BF16),
            pltpu.VMEM((1, width), F32),
            pltpu.VMEM((rows_here, width_q), BF16),
            pltpu.VMEM((rows_here, kv_width), BF16),
            pltpu.VMEM((rows_here, kv_width), BF16),
            pltpu.VMEM((2, table_rows(rows_here), 128), F32),
            pltpu.VMEM((2, WINDOW, 128), F32),
            pltpu.VMEM((kv_local, reach, HEAD_DIM), BF16),
            pltpu.VMEM((kv_local, reach, HEAD_DIM), BF16),
            pltpu.VMEM((4, WINDOW, kv_width), BF16),
            pltpu.VMEM((rows_here, width_q), BF16),
            pltpu.VMEM((n_tp, rows_here // n_tp, width_q), BF16),
            pltpu.VMEM((n_z, 2 * top_count, tok), F32),
            pltpu.VMEM((n_z, PANELS, tok, panel), BF16),
            pltpu.VMEM((slots, tok), BF16),
            pltpu.VMEM((n_z, PANELS, slots, panel), BF16),
            pltpu.VMEM((n_z, PANELS, slots, panel), BF16),
            pltpu.VMEM((n_z, PANELS, slots, panel), BF16),
            pltpu.VMEM((n_z, PANELS, slots, panel), BF16),
            pltpu.VMEM((n_z, 2, tok, slots), BF16),
            pltpu.VMEM((n_z, PANELS, tok, panel), BF16),
            pltpu.VMEM((n_z + 1, PANELS, tok, panel), BF16),
            pltpu.VMEM((width, hidden), BF16),
            pltpu.VMEM((width, hidden), BF16),
            pltpu.VMEM((hidden, width), BF16),
            pltpu.VMEM(mix_weight.shape, BF16),
            pltpu.VMEM((slots, hidden), BF16),
            dma((n_z + 1, PANELS)),
            both,
            dma((n_z,)),
            dma((n_z,)),
            both,
            both,
            both,
            both,
            both,
            dma((n_z + 1, PANELS)),
            dma,
            dma,
            dma((4,)),
            dma((4,)),
            dma((14,)),
        ],
        compiler_params=pltpu.CompilerParams(
            collective_id=0, has_side_effects=True, vmem_limit_bytes=VMEM_BYTES
        ),
        name="layer",
    )(
        sink_logits,
        routes.T,
        route_weights.T,
        expert_input,
        norm_gain[None, :],
        queries,
        key_heads,
        value_heads,
        tables,
        gate_weight,
        up_weight,
        down_weight,
        mix_weight,
    )


def z_count(mesh, n_ep):
    coords = {getattr(d, "coords", (0, 0, 0))[2] for d in mesh.devices.flat}
    return len(coords) if len(coords) in (2, 4) and n_ep % len(coords) == 0 else 1


def solution(mesh):
    n_ep, n_tp = mesh.shape["ep"], mesh.shape["tp"]
    n_z = z_count(mesh, n_ep)
    grid = Mesh(mesh.devices.reshape(n_z, n_ep // n_z, n_tp), ("zz", "xx", "tp"))
    ep = ("zz", "xx")
    every = ("zz", "xx", "tp")
    return jax.shard_map(
        body,
        mesh=grid,
        in_specs=(
            P(ep, "tp"),
            P(ep, "tp"),
            P(ep, "tp"),
            P("tp"),
            P(),
            P(every, None),
            P(),
            P(every, None),
            P(every, None),
            P(every, None, None),
            P(every, None, None),
            P(every, None, None),
        ),
        out_specs=(P(every, None), P(every, None)),
        check_vma=False,
    )
```

```python
import functools

import jax
import jax.numpy as jnp
import numpy as np
from jax import lax
from jax.experimental import pallas as pl
from jax.experimental.pallas import tpu as pltpu
from jax.sharding import Mesh
from jax.sharding import PartitionSpec as P

HEAD_DIM = 64
WINDOW = 128
GRID_W = 64
ROPE_BASE = 10000.0
CLAMP_LIMIT = 7.0
GATE_SLOPE = 1.702
NORM_EPS = 1e-05

F32 = jnp.float32
BF16 = jnp.bfloat16
MESH = pl.DeviceIdType.MESH
PANELS = 2
TILE = 256
RELAYED = 256
VMEM_BYTES = 61 << 20

scope = jax.named_scope


def table_rows(rows_here):
    return -(-(rows_here + 2 * WINDOW) // GRID_W // 8) * 8


def angle_tables(length, rows_here):
    half = HEAD_DIM // 2
    quarter = HEAD_DIM // 4
    lane = np.arange(2 * HEAD_DIM) % HEAD_DIM
    freqs = (ROPE_BASE ** (-np.arange(0, half, 2) / half)).astype(np.float32)
    lane_freq = np.tile(freqs, 2 * HEAD_DIM // quarter)
    count = (length - rows_here) // GRID_W + table_rows(rows_here)
    by_row = np.arange(count) - WINDOW // GRID_W
    by_col = np.arange(WINDOW) % GRID_W
    place = np.concatenate([by_row, by_col]).astype(np.float32)
    angle = (place[:, None] * lane_freq[None, :]).astype(np.float64)
    sign = np.where(lane % half < quarter, -1.0, 1.0)
    return np.stack([np.cos(angle), np.sin(angle) * sign]).astype(np.float32)


def turn(cells, cosines, sines):
    quarter = HEAD_DIM // 4
    width = cells.shape[1]
    lane = lax.broadcasted_iota(jnp.int32, cells.shape, 1)
    ahead = pltpu.roll(cells, width - quarter, 1)
    behind = pltpu.roll(cells, quarter, 1)
    partner = jnp.where(lane % (2 * quarter) < quarter, ahead, behind)
    return cells * cosines + partner * sines

def kernel(
    sizes,
    sink_hbm,
    route_hbm,
    share_hbm,
    x_hbm,
    gain_hbm,
    q_hbm,
    k_hbm,
    v_hbm,
    table_hbm,
    wg_hbm,
    wu_hbm,
    wd_hbm,
    mix_hbm,
    mixer_ref,
    expert_ref,
    sink,
    route_ref,
    share_ref,
    x_ref,
    gain_ref,
    q_ref,
    k_ref,
    v_ref,
    by_row,
    by_col,
    k_scr,
    v_scr,
    halo,
    att,
    att_in,
    routing,
    normed,
    picks,
    outgoing,
    arrived,
    produced,
    returned,
    shares,
    partial,
    home,
    relayed,
    relay_shares,
    relay_sum,
    relay_home,
    crossed,
    wg,
    wu,
    wd,
    mix,
    act,
    z_send,
    z_recv,
    rt_send,
    rt_recv,
    out_send,
    out_recv,
    back_send,
    back_recv,
    home_send,
    home_recv,
    relay_send,
    relay_recv,
    sum_send,
    sum_recv,
    cross_send,
    cross_recv,
    att_send,
    att_recv,
    halo_send,
    halo_recv,
    load_sem,
):
    n_z, n_x, n_y, n_tp, top_count, capacity = sizes
    n_ep = n_z * n_x
    plane = n_x * n_tp
    slots = plane * capacity
    cores = n_tp // n_y
    side = n_x * cores
    z, x, t = lax.axis_index("zz"), lax.axis_index("xx"), lax.axis_index("tp")
    me = x * n_tp + t
    y, core = lax.div(t, cores), lax.rem(t, cores)
    ep = z * n_x + x
    rows_here, width_q = q_ref.shape
    tok, width = x_ref.shape
    panel = width // PANELS
    back_width = [panel] * (PANELS - 1) + [panel - RELAYED]
    relay_cols = pl.ds(panel - RELAYED, RELAYED)
    length = rows_here * n_ep
    kv_local = k_scr.shape[0]
    bq = WINDOW
    span = bq + 2 * WINDOW
    blocks = rows_here // bq
    chunk = rows_here // n_tp
    last = n_z - 1
    grid_rows = by_row.shape[1]
    table_end = table_hbm.shape[1] - WINDOW

    def z_dev(b):
        return (b, x, t)

    def plane_dev(p):
        return (z, lax.div(p, n_tp), lax.rem(p, n_tp))

    def ep_dev(e):
        return (lax.div(e, n_x), lax.rem(e, n_x), t)

    after, before = lax.rem(ep + 1, n_ep), lax.rem(ep + n_ep - 1, n_ep)
    has_after, has_before = ep < n_ep - 1, ep > 0
    has_up, has_down = z < last, z > 0
    end = (z == 0) | (z == last)
    mid = (z > 0) & (z < last)

    closer = jnp.minimum(z, last - z)
    far_side = jnp.where(z < last - z, 1, -1)

    def nearest(i):
        if i == 0:
            return z
        paired = z + ((i + 1) // 2) * (-1 if i % 2 else 1)
        return jnp.where(i <= 2 * closer, paired, z + far_side * (i - closer))

    def going_back(i):
        return lax.bitwise_xor(z, jnp.int32(last - i))

    first_row = pl.multiple_of(ep * (rows_here // GRID_W), 8)
    loads = {
        "route": (route_hbm, route_ref),
        "share": (share_hbm, share_ref),
        "x": (x_hbm, x_ref),
        "gain": (gain_hbm, gain_ref),
        "sink": (sink_hbm, sink),
        "k": (k_hbm, k_ref),
        "v": (v_hbm, v_ref),
        "by_row": (table_hbm.at[:, pl.ds(first_row, grid_rows)], by_row),
        "by_col": (table_hbm.at[:, pl.ds(table_end, WINDOW)], by_col),
        "q": (q_hbm, q_ref),
        "wg": (wg_hbm.at[0], wg),
        "wu": (wu_hbm.at[0], wu),
        "wd": (wd_hbm.at[0], wd),
        "mix": (mix_hbm, mix),
    }
    loads = {
        name: pltpu.make_async_copy(source, target, load_sem.at[i])
        for i, (name, (source, target)) in enumerate(loads.items())
    }
    for load in loads.values():
        load.start()

    def loaded(*names):
        for name in names:
            loads[name].wait()

    barrier = pltpu.get_barrier_semaphore()

    def greet_z(o, _):
        pl.semaphore_signal(barrier, inc=1, device_id=z_dev(lax.rem(z + o, n_z)), device_id_type=MESH)
        return 0

    def greet_plane(p, _):
        pl.semaphore_signal(
            barrier, inc=1, device_id=plane_dev(lax.rem(me + p, plane)), device_id_type=MESH
        )
        return 0

    def column(o):
        b, row = lax.rem(z + o // n_y, n_z), lax.rem(y + o % n_y, n_y)
        return (b, x, row * cores + core)

    lax.fori_loop(1, n_z, greet_z, 0)
    for o in range(n_y + 1, n_z * n_y):
        if o % n_y:
            pl.semaphore_signal(barrier, inc=1, device_id=column(o), device_id_type=MESH)
    lax.fori_loop(1, plane, greet_plane, 0)
    for e in (after, before):
        pl.semaphore_signal(barrier, inc=1, device_id=ep_dev(e), device_id_type=MESH)

    def await_bytes(ref, sem):
        pltpu.make_async_copy(ref, ref, sem).wait()

    upper = (
        lax.broadcasted_iota(jnp.int32, (tok, tok), 0) < lax.broadcasted_iota(jnp.int32, (tok, tok), 1)
    ).astype(F32).astype(BF16)

    def pick_rows(route, expert_of_slot, count):
        slot_row = lax.broadcasted_iota(jnp.int32, (count, tok), 0)
        lane_expert = expert_of_slot(lax.div(slot_row, capacity)).astype(F32)
        place_in = lax.rem(slot_row, capacity).astype(F32)
        member = jnp.zeros((count, tok), F32)
        share = jnp.zeros((count, tok), F32)
        for k in range(top_count):
            hit = route[k : k + 1, :] == lane_expert
            member = jnp.where(hit, 1.0, member)
            share = jnp.where(hit, route[top_count + k : top_count + k + 1, :], share)
        rank = jnp.dot(member.astype(BF16), upper, preferred_element_type=F32)
        pick = jnp.where(rank == place_in, member, 0.0)
        scaled = (share * pick).T
        coarse = scaled.astype(BF16)
        return pick, coarse, (scaled - coarse.astype(F32)).astype(BF16)

    def choose(i):
        b = nearest(i)
        if i > 0:
            await_bytes(routing.at[b, y], rt_recv.at[b, y])
        pick, coarse, fine = pick_rows(routing[b, y], lambda e: z * plane + e, slots)
        picks[...] = pick.astype(BF16)
        shares[b, 0] = coarse
        shares[b, 1] = fine

    def choose_relayed(i):
        b = nearest(i)

        def expert(e):
            return z * plane + lax.div(e, cores) * n_tp + y * cores + lax.rem(e, cores)

        for o in range(n_y):
            row = lax.rem(y + o, n_y)
            if o > 0:
                await_bytes(routing.at[b, row], rt_recv.at[b, row])
            _, coarse, fine = pick_rows(routing[b, row], expert, side * capacity)
            relay_shares[b, row, 0] = coarse
            relay_shares[b, row, 1] = fine

    loaded("route", "share")
    routing[z, y, :top_count, :] = route_ref[...].astype(F32)
    routing[z, y, top_count:, :] = share_ref[...]
    choose(0)
    loaded("x", "gain")
    with scope("norm"):
        for part in range(tok // 32):
            rows = slice(part * 32, part * 32 + 32)
            values = x_ref[rows, :].astype(F32)
            center = jnp.mean(values, axis=1, keepdims=True)
            spread = jnp.mean(jnp.square(values - center), axis=1, keepdims=True)
            result = ((values - center) * lax.rsqrt(spread + NORM_EPS) * gain_ref[...]).astype(BF16)
            for h in range(PANELS):
                normed[z, h, rows, :] = result[:, h * panel : h * panel + panel]
    with scope("barr"):
        pl.semaphore_wait(barrier, (n_z - 1) * n_y + plane - 1 + 2)

    def rt_copy(o):
        return pltpu.make_async_remote_copy(
            src_ref=routing.at[z, y],
            dst_ref=routing.at[z, y],
            send_sem=rt_send.at[o],
            recv_sem=rt_recv.at[z, y],
            device_id=column(o),
            device_id_type=MESH,
        )

    def z_copy(i, h, b, target):
        return pltpu.make_async_remote_copy(
            src_ref=normed.at[b, h],
            dst_ref=normed.at[b, h],
            send_sem=z_send.at[i, h],
            recv_sem=z_recv.at[b, h],
            device_id=z_dev(target),
            device_id_type=MESH,
        )

    def onward(i):
        b = nearest(i)
        target = jnp.where(b < z, z + 1, z - 1)
        return b, target, (target >= 0) & (target <= last)

    for o in range(1, n_z * n_y):
        rt_copy(o).start()
    if n_z > 1:
        for h in range(PANELS):

            @pl.when(has_up)
            def _():
                z_copy(0, h, z, z + 1).start()

            @pl.when(has_down)
            def _():
                z_copy(n_z, h, z, z - 1).start()

    def tick(distance, h):
        for i in range(1, n_z):
            if not (i + 1) // 2 <= distance <= i:
                continue
            b, target, goes_on = onward(i)

            @pl.when(jnp.abs(b - z) == distance)
            def _():
                with scope(f"zwait{i}{h}"):
                    await_bytes(normed.at[b, h], z_recv.at[b, h])

                @pl.when(goes_on)
                def _():
                    z_copy(i, h, b, target).start()

    def dispatch(i, h):
        b = nearest(i)
        with scope(f"disp{i}{h}"):
            if h == 0 and i > 0:
                choose(i)

            def tile(j, _):
                cols = pl.ds(pl.multiple_of(j * TILE, TILE), TILE)
                outgoing[b, h, :, cols] = jnp.dot(
                    picks[...], normed[b, h, :, cols], preferred_element_type=F32
                ).astype(BF16)
                return 0

            lax.fori_loop(0, panel // TILE, tile, 0)
            exchange(outgoing, arrived, out_send, out_recv, b, h, panel)

    def exchange(source, target, send, recv, b, h, count):
        mine = pl.ds(pl.multiple_of(me * capacity, capacity), capacity)
        cols = pl.ds(0, count)

        def one(p, _):
            to = lax.rem(me + p, plane)
            pltpu.make_async_remote_copy(
                src_ref=source.at[b, h, pl.ds(pl.multiple_of(to * capacity, capacity), capacity), cols],
                dst_ref=target.at[b, h, mine, cols],
                send_sem=send.at[b, h],
                recv_sem=recv.at[b, h],
                device_id=plane_dev(to),
                device_id_type=MESH,
            ).start()
            return 0

        lax.fori_loop(1, plane, one, 0)
        pltpu.make_async_copy(
            source.at[b, h, mine, cols], target.at[b, h, mine, cols], recv.at[b, h]
        ).start()

    def halo_copy(source, which, start, target):
        return pltpu.make_async_remote_copy(
            src_ref=source.at[pl.ds(start, WINDOW)],
            dst_ref=halo.at[which],
            send_sem=halo_send.at[which],
            recv_sem=halo_recv.at[which],
            device_id=ep_dev(target),
            device_id_type=MESH,
        )

    to_after = [
        halo_copy(k_ref, 0, rows_here - WINDOW, after),
        halo_copy(v_ref, 1, rows_here - WINDOW, after),
    ]
    to_before = [halo_copy(k_ref, 2, 0, before), halo_copy(v_ref, 3, 0, before)]

    def send_halos():
        for there, copies in ((has_after, to_after), (has_before, to_before)):

            @pl.when(there)
            def _():
                for copy in copies:
                    copy.start()

    def await_halos():
        for there, copies in ((has_before, to_after), (has_after, to_before)):

            @pl.when(there)
            def _():
                for copy in copies:
                    copy.wait_recv()

        for there, which in ((has_before, 0), (has_after, 2)):

            @pl.when(jnp.logical_not(there))
            def _():
                halo[which] = jnp.zeros(halo.shape[1:], BF16)
                halo[which + 1] = jnp.zeros(halo.shape[1:], BF16)

    of_row = lax.rem(lax.broadcasted_iota(jnp.int32, (WINDOW, 128), 1), HEAD_DIM) < HEAD_DIM // 2

    def angles(which, at):
        start = lax.div(at, GRID_W)
        parts = [
            jnp.broadcast_to(by_row[which, pl.ds(start + i, 1), :], (GRID_W, 128))
            for i in range(WINDOW // GRID_W)
        ]
        return jnp.where(of_row, jnp.concatenate(parts, axis=0), by_col[which])

    def place(source, values, at, count):
        cosines, sines = angles(0, at), angles(1, at)
        for pair in range(kv_local // 2):
            cols = slice(pair * 128, pair * 128 + 128)
            turned = turn(source[:, cols].astype(F32), cosines, sines).astype(BF16)
            piece = values[:, cols]
            for side in range(2):
                lanes = slice(side * 64, side * 64 + 64)
                k_scr[2 * pair + side, pl.ds(at, count), :] = turned[:, lanes]
                v_scr[2 * pair + side, pl.ds(at, count), :] = piece[:, lanes]

    def place_own(i, _):
        at = pl.multiple_of(i * 128, 128)
        place(k_ref[pl.ds(at, 128), :], v_ref[pl.ds(at, 128), :], WINDOW + at, 128)
        return 0

    row = lax.rem(lax.broadcasted_iota(jnp.int32, (2 * bq, span), 0), bq)
    col = lax.broadcasted_iota(jnp.int32, (2 * bq, span), 1)
    top = lax.broadcasted_iota(jnp.int32, (2 * bq, 1), 0) < bq

    def attend(block, _):
        first = pl.multiple_of(block * bq, bq)
        cosines = angles(0, first + WINDOW) * HEAD_DIM**-0.5
        sines = angles(1, first + WINDOW) * HEAD_DIM**-0.5
        key_pos = ep * rows_here + first - WINDOW + col
        inside = (col >= row) & (col <= row + 2 * WINDOW) & (key_pos >= 0) & (key_pos < length)
        for g in range(kv_local):
            q = q_ref[pl.ds(first, bq), g * 128 : g * 128 + 128].astype(F32)
            q = turn(q, cosines, sines).astype(BF16)
            q2 = jnp.concatenate([q[:, :64], q[:, 64:]], axis=0)
            k = k_scr[g, pl.ds(first, span), :]
            v = v_scr[g, pl.ds(first, span), :]
            scores = lax.dot_general(q2, k, (((1,), (1,)), ((), ())), preferred_element_type=F32)
            scores = jnp.where(inside, scores, -jnp.inf)
            logit = jnp.where(top, sink[2 * g], sink[2 * g + 1])
            peak = jnp.maximum(jnp.max(scores, axis=1, keepdims=True), logit)
            weights = jnp.exp(scores - peak)
            total = jnp.sum(weights, axis=1, keepdims=True) + jnp.exp(logit - peak)
            chances = (weights * (1.0 / total)).astype(BF16)
            blend = jnp.dot(chances, v, preferred_element_type=F32).astype(BF16)
            att[pl.ds(first, bq), g * 128 : g * 128 + 128] = jnp.concatenate(
                [blend[:bq], blend[bq:]], axis=1
            )
        return 0

    def attend_inner(part, parts):
        inner = blocks - 2
        with scope(f"att{part}"):
            lax.fori_loop(1 + inner * part // parts, 1 + inner * (part + 1) // parts, attend, 0)

    def attend_edges():
        with scope("halowait"):
            await_halos()
        with scope("edges"):
            place(halo[0], halo[1], 0, WINDOW)
            place(halo[2], halo[3], WINDOW + rows_here, WINDOW)
            lax.fori_loop(0, 2, lambda i, _: attend(i * (blocks - 1), _), 0)

    def send_heads(edges):
        each = chunk // bq

        def one(p, _):
            to = lax.rem(t + p, n_tp)
            for i in range(each):
                block = to * each + i
                at_edge = (block == 0) | (block == blocks - 1)

                @pl.when(at_edge if edges else jnp.logical_not(at_edge))
                def _():
                    pltpu.make_async_remote_copy(
                        src_ref=att.at[pl.ds(pl.multiple_of(block * bq, bq), bq)],
                        dst_ref=att_in.at[t, i * bq : i * bq + bq],
                        send_sem=att_send,
                        recv_sem=att_recv,
                        device_id=(z, x, to),
                        device_id_type=MESH,
                    ).start()

            return 0

        lax.fori_loop(1, n_tp, one, 0)
        if edges:
            own = pl.ds(pl.multiple_of(t * chunk, chunk), chunk)
            pltpu.make_async_copy(att.at[own], att_in.at[t], att_recv).start()

    def mixer():
        with scope("attwait"):
            await_bytes(att_in, att_recv)
        loaded("mix")

        def tile(j, _):
            cols = pl.ds(pl.multiple_of(j * TILE, TILE), TILE)
            total = jnp.zeros((chunk, TILE), F32)
            for s in range(n_tp):
                total = total + jnp.dot(
                    att_in[s], mix[s * width_q : s * width_q + width_q, cols], preferred_element_type=F32
                )
            mixer_ref[:, cols] = total.astype(BF16)
            return 0

        with scope("mixer"):
            lax.fori_loop(0, width // TILE, tile, 0)

    def experts(i, sent=lambda h: None):
        b = nearest(i)
        hidden = wg.shape[1]
        for h in range(PANELS):
            with scope(f"arrwait{i}{h}"):
                await_bytes(arrived.at[b, h], out_recv.at[b, h])

        def up(j, _):
            cols = pl.ds(pl.multiple_of(j * TILE, TILE), TILE)
            gate = jnp.zeros((slots, TILE), F32)
            lift = jnp.zeros((slots, TILE), F32)
            for h in range(PANELS):
                rows = arrived[b, h]
                deep = slice(h * panel, h * panel + panel)
                gate = gate + jnp.dot(rows, wg[deep, cols], preferred_element_type=F32)
                lift = lift + jnp.dot(rows, wu[deep, cols], preferred_element_type=F32)
            gate = jnp.minimum(gate, CLAMP_LIMIT)
            lift = jnp.clip(lift, -CLAMP_LIMIT, CLAMP_LIMIT)
            act[:, cols] = ((lift + 1.0) * gate * jax.nn.sigmoid(GATE_SLOPE * gate)).astype(BF16)
            return 0

        with scope(f"exp{i}"):
            lax.fori_loop(0, hidden // TILE, up, 0)
            for h in range(PANELS):

                def down(j, _):
                    cols = pl.ds(pl.multiple_of(j * TILE, TILE), TILE)
                    wide = pl.ds(pl.multiple_of(h * panel + j * TILE, TILE), TILE)
                    produced[b, h, :, cols] = jnp.dot(
                        act[...], wd[:, wide], preferred_element_type=F32
                    ).astype(BF16)
                    return 0

                lax.fori_loop(0, panel // TILE, down, 0)
                sent(h)

    def send_back(b, h):
        exchange(produced, returned, back_send, back_recv, b, h, back_width[h])

    def send_relayed(b):
        mine = pl.ds(pl.multiple_of((x * cores + core) * capacity, capacity), capacity)

        def source(to, row):
            slot = lax.div(to, cores) * n_tp + row * cores + lax.rem(to, cores)
            rows = pl.ds(pl.multiple_of(slot * capacity, capacity), capacity)
            return produced.at[b, PANELS - 1, rows, relay_cols]

        def one(p, _):
            to = lax.rem(x * cores + core + p, side)
            for row in range(n_y):
                pltpu.make_async_remote_copy(
                    src_ref=source(to, row),
                    dst_ref=relayed.at[b, row, mine],
                    send_sem=relay_send.at[b],
                    recv_sem=relay_recv.at[b],
                    device_id=(z, lax.div(to, cores), y * cores + lax.rem(to, cores)),
                    device_id_type=MESH,
                ).start()
            return 0

        lax.fori_loop(1, side, one, 0)
        for row in range(n_y):
            pltpu.make_async_copy(
                source(x * cores + core, row), relayed.at[b, row, mine], relay_recv.at[b]
            ).start()

    def homeward(b):
        target = jnp.where(b < z, z - 1, z + 1)
        return target, jnp.where((target == b) & (b < z), n_z, b)

    def home_copy(b, h):
        target, slot = homeward(b)
        cols = pl.ds(0, back_width[h])
        return pltpu.make_async_remote_copy(
            src_ref=partial.at[b, h, :, cols],
            dst_ref=home.at[slot, h, :, cols],
            send_sem=home_send.at[b, h],
            recv_sem=home_recv.at[slot, h],
            device_id=z_dev(target),
            device_id_type=MESH,
        )

    def relay_copy(b):
        target, slot = homeward(b)
        return pltpu.make_async_remote_copy(
            src_ref=relay_sum.at[b],
            dst_ref=relay_home.at[slot],
            send_sem=sum_send.at[b],
            recv_sem=sum_recv.at[slot],
            device_id=z_dev(target),
            device_id_type=MESH,
        )

    def cross_copy(o):
        row = lax.rem(y + o, n_y)
        return pltpu.make_async_remote_copy(
            src_ref=relay_sum.at[z, row],
            dst_ref=crossed.at[y],
            send_sem=cross_send.at[o],
            recv_sem=cross_recv.at[y],
            device_id=(z, x, row * cores + core),
            device_id_type=MESH,
        )

    def clear_home():
        for slot, missing in ((z, z == 0), (n_z, z == last)):

            @pl.when(missing)
            def _():
                home[slot] = jnp.zeros(home.shape[1:], BF16)
                relay_home[slot] = jnp.zeros(relay_home.shape[1:], BF16)

    def weighted(b, h, cols):
        rows = returned[b, h, :, cols]
        total = jnp.dot(shares[b, 0], rows, preferred_element_type=F32)
        return total + jnp.dot(shares[b, 1], rows, preferred_element_type=F32)

    def relay_weighted(b, row):
        rows = relayed[b, row]
        total = jnp.dot(relay_shares[b, row, 0], rows, preferred_element_type=F32)
        return total + jnp.dot(relay_shares[b, row, 1], rows, preferred_element_type=F32)

    def combine_relayed(name, b, further):
        with scope(f"relwait{name}"):
            await_bytes(relayed.at[b], relay_recv.at[b])
            if further:
                await_bytes(relay_home.at[b], sum_recv.at[b])

        with scope(f"rel{name}"):
            for row in range(n_y):
                total = relay_weighted(b, row)
                if further:
                    total = total + relay_home[b, row].astype(F32)
                relay_sum[b, row] = total.astype(BF16)
        relay_copy(b).start()

    def from_both_sides(place, sem):
        @pl.when(has_down)
        def _():
            await_bytes(place(z), sem(z))

        @pl.when(has_up)
        def _():
            await_bytes(place(n_z), sem(n_z))

    def combine_own_relayed():
        with scope("relwaitown"):
            await_bytes(relayed.at[z], relay_recv.at[z])
            from_both_sides(lambda slot: relay_home.at[slot], lambda slot: sum_recv.at[slot])
        for row in range(n_y):
            total = relay_weighted(z, row) + relay_home[z, row].astype(F32)
            relay_sum[z, row] = (total + relay_home[n_z, row].astype(F32)).astype(BF16)
        for o in range(1, n_y):
            cross_copy(o).start()

    def finish_relayed():
        total = relay_sum[z, y].astype(F32)
        for o in range(1, n_y):
            row = lax.rem(y + o, n_y)
            with scope("crosswait"):
                await_bytes(crossed.at[row], cross_recv.at[row])
            total = total + crossed[row].astype(F32)
        expert_ref[:, width - RELAYED :] = total.astype(BF16)

    def combine(name, b, h, further):
        cols = pl.ds(0, back_width[h])
        with scope(f"retwait{name}"):
            await_bytes(returned.at[b, h, :, cols], back_recv.at[b, h])

        if further:
            with scope(f"chain{name}"):
                await_bytes(home.at[b, h, :, cols], home_recv.at[b, h])

        def tile(j, _):
            cols = pl.ds(pl.multiple_of(j * TILE, TILE), TILE)
            total = weighted(b, h, cols)
            if further:
                total = total + home[b, h, :, cols].astype(F32)
            partial[b, h, :, cols] = total.astype(BF16)
            return 0

        with scope(f"comb{name}"):
            lax.fori_loop(0, back_width[h] // TILE, tile, 0)
        home_copy(b, h).start()

    def combine_own(h):
        here = pl.ds(0, back_width[h])
        with scope(f"retwaitown{h}"):
            await_bytes(returned.at[z, h, :, here], back_recv.at[z, h])
        with scope(f"homewait{h}"):
            from_both_sides(lambda slot: home.at[slot, h, :, here], lambda slot: home_recv.at[slot, h])

        def tile(j, _):
            cols = pl.ds(pl.multiple_of(j * TILE, TILE), TILE)
            wide = pl.ds(pl.multiple_of(h * panel + j * TILE, TILE), TILE)
            total = weighted(z, h, cols) + home[z, h, :, cols].astype(F32)
            total = total + home[n_z, h, :, cols].astype(F32)
            expert_ref[:, wide] = total.astype(BF16)
            return 0

        with scope(f"combown{h}"):
            lax.fori_loop(0, back_width[h] // TILE, tile, 0)

    for h in range(PANELS):
        dispatch(0, h)
    clear_home()
    loaded("k", "v", "by_row", "by_col", "q", "sink")
    with scope("place"):
        lax.fori_loop(0, rows_here // 128, place_own, 0)
    attend_inner(0, 3)
    for h in range(PANELS):
        if n_z > 1:
            tick(1, h)
            dispatch(1, h)
        attend_inner(1 + h, 3)
    if n_z > 2:
        tick(2, 0)
        dispatch(2, 0)
    loaded("wg", "wu", "wd")
    if n_z > 1:
        experts(0)
    if n_z > 2:
        tick(2, 1)
        dispatch(2, 1)
        experts(1)
        for h in range(PANELS):
            tick(3, h)
            dispatch(3, h)
    send_halos()
    send_heads(False)
    if n_z > 1:
        send_relayed(z)
    if n_z > 2:
        send_relayed(nearest(1))
    with scope("chooserel"):
        for i in range(n_z):
            choose_relayed(i)
    if n_z > 2:
        experts(2)
        send_relayed(nearest(2))

        @pl.when(mid)
        def _():
            for h in range(PANELS):
                send_back(going_back(0), h)

    def sent(h):
        if h == PANELS - 1:
            send_relayed(nearest(last))

        @pl.when(end)
        def _():
            send_back(going_back(0), h)

    experts(last, sent)
    attend_edges()
    send_heads(True)
    for i in range(1, n_z):
        for h in range(PANELS):
            send_back(going_back(i), h)
    firsts, then = [(i, None) for i in (*range(1, last), 0)][: max(last, 0)], []
    if n_z > 1:
        firsts += [(0, h) for h in range(PANELS)]
        then = [(i, h) for i in range(1, last) for h in range(PANELS)]

    def sums(steps, further):
        for i, h in steps:
            if h is None:
                combine_relayed(i, going_back(i), further)
            else:
                combine(f"{i}{h}", going_back(i), h, further)

    if n_z > 2:

        @pl.when(mid)
        def _():
            sums([(0, None), (1, None)], True)

        @pl.when(end)
        def _():
            sums(firsts, False)

        mixer()

        @pl.when(mid)
        def _():
            later = [(i, h) for h in range(PANELS) for i in (2, 0)]
            sums([(2, None)] + [(1, h) for h in range(PANELS)] + later, True)

        @pl.when(end)
        def _():
            sums(then, False)
    else:
        sums(firsts, False)
        mixer()
    combine_own_relayed()
    for o in range(1, n_z * n_y):
        rt_copy(o).wait_send()
    if n_z > 1:
        for h in range(PANELS):

            @pl.when(has_up)
            def _():
                z_copy(0, h, z, z + 1).wait_send()

            @pl.when(has_down)
            def _():
                z_copy(n_z, h, z, z - 1).wait_send()

            for i in range(1, n_z):
                b, target, goes_on = onward(i)

                @pl.when(goes_on)
                def _():
                    z_copy(i, h, b, target).wait_send()
    for there, copies in ((has_after, to_after), (has_before, to_before)):

        @pl.when(there)
        def _():
            for copy in copies:
                copy.wait_send()

    for b in range(n_z):
        for h in range(PANELS):
            gone = pl.ds(0, (plane - 1) * capacity)
            await_bytes(outgoing.at[b, h, gone], out_send.at[b, h])
        gone = pl.ds(0, (side - 1) * n_y * capacity)
        await_bytes(produced.at[b, 0, gone, pl.ds(0, RELAYED)], relay_send.at[b])
    await_bytes(att.at[pl.ds(0, (n_tp - 1) * chunk)], att_send)

    for h in range(PANELS):
        combine_own(h)
        if h == 0:
            finish_relayed()

    with scope("late"):
        for h in range(PANELS):
            for i in range(1, n_z):
                home_copy(nearest(i), h).wait_send()
            for b in range(n_z):
                gone = pl.ds(0, (plane - 1) * capacity)
                await_bytes(produced.at[b, h, gone, pl.ds(0, back_width[h])], back_send.at[b, h])
        for i in range(1, n_z):
            relay_copy(nearest(i)).wait_send()
        for o in range(1, n_y):
            cross_copy(o).wait_send()


def hand_over(mixer_in, expert_in, mixer_out, expert_out, sem):
    copies = [
        pltpu.make_async_copy(source, target, sem.at[i])
        for i, (source, target) in enumerate(((mixer_in, mixer_out), (expert_in, expert_out)))
    ]
    for copy in copies:
        copy.start()
    for copy in copies:
        copy.wait()


def body(
    n_y,
    queries,
    key_heads,
    value_heads,
    sink_logits,
    mix_weight,
    expert_input,
    norm_gain,
    routes,
    route_weights,
    gate_weight,
    up_weight,
    down_weight,
):
    n_z, n_x, n_tp = lax.axis_size("zz"), lax.axis_size("xx"), lax.axis_size("tp")
    n_ep = n_z * n_x
    plane = n_x * n_tp
    rows_here, width_q = queries.shape
    kv_width = key_heads.shape[1]
    kv_local = kv_width // HEAD_DIM
    tok, top_count = routes.shape
    capacity = 2 * tok * top_count // (n_ep * n_tp)
    slots = plane * capacity
    width = expert_input.shape[1]
    panel = width // PANELS
    hidden = gate_weight.shape[2]
    tables = jnp.asarray(angle_tables(rows_here * n_ep, rows_here))
    anywhere = pl.BlockSpec(memory_space=pl.ANY)
    vmem = pl.BlockSpec(memory_space=pltpu.VMEM)
    reach = rows_here + 2 * WINDOW
    dma = pltpu.SemaphoreType.DMA
    shapes = [
        jax.ShapeDtypeStruct((rows_here // n_tp, width), BF16),
        jax.ShapeDtypeStruct((tok, width), BF16),
    ]
    both = dma((n_z, PANELS))
    side_slots = slots // n_y
    mixed, expert = pl.pallas_call(
        functools.partial(kernel, (n_z, n_x, n_y, n_tp, top_count, capacity)),
        in_specs=[anywhere] * 13,
        out_specs=[vmem] * 2,
        out_shape=[pltpu.VMEM(s.shape, s.dtype) for s in shapes],
        scratch_shapes=[
            pltpu.SMEM(sink_logits.shape, F32),
            pltpu.VMEM((top_count, tok), jnp.int32),
            pltpu.VMEM((top_count, tok), F32),
            pltpu.VMEM((tok, width), BF16),
            pltpu.VMEM((1, width), F32),
            pltpu.VMEM((rows_here, width_q), BF16),
            pltpu.VMEM((rows_here, kv_width), BF16),
            pltpu.VMEM((rows_here, kv_width), BF16),
            pltpu.VMEM((2, table_rows(rows_here), 128), F32),
            pltpu.VMEM((2, WINDOW, 128), F32),
            pltpu.VMEM((kv_local, reach, HEAD_DIM), BF16),
            pltpu.VMEM((kv_local, reach, HEAD_DIM), BF16),
            pltpu.VMEM((4, WINDOW, kv_width), BF16),
            pltpu.VMEM((rows_here, width_q), BF16),
            pltpu.VMEM((n_tp, rows_here // n_tp, width_q), BF16),
            pltpu.VMEM((n_z, n_y, 2 * top_count, tok), F32),
            pltpu.VMEM((n_z, PANELS, tok, panel), BF16),
            pltpu.VMEM((slots, tok), BF16),
            pltpu.VMEM((n_z, PANELS, slots, panel), BF16),
            pltpu.VMEM((n_z, PANELS, slots, panel), BF16),
            pltpu.VMEM((n_z, PANELS, slots, panel), BF16),
            pltpu.VMEM((n_z, PANELS, slots, panel), BF16),
            pltpu.VMEM((n_z, 2, tok, slots), BF16),
            pltpu.VMEM((n_z, PANELS, tok, panel), BF16),
            pltpu.VMEM((n_z + 1, PANELS, tok, panel), BF16),
            pltpu.VMEM((n_z, n_y, side_slots, RELAYED), BF16),
            pltpu.VMEM((n_z, n_y, 2, tok, side_slots), BF16),
            pltpu.VMEM((n_z, n_y, tok, RELAYED), BF16),
            pltpu.VMEM((n_z + 1, n_y, tok, RELAYED), BF16),
            pltpu.VMEM((n_y, tok, RELAYED), BF16),
            pltpu.VMEM((width, hidden), BF16),
            pltpu.VMEM((width, hidden), BF16),
            pltpu.VMEM((hidden, width), BF16),
            pltpu.VMEM(mix_weight.shape, BF16),
            pltpu.VMEM((slots, hidden), BF16),
            dma((n_z + 1, PANELS)),
            both,
            dma((n_z * n_y,)),
            dma((n_z, n_y)),
            both,
            both,
            both,
            both,
            both,
            dma((n_z + 1, PANELS)),
            dma((n_z,)),
            dma((n_z,)),
            dma((n_z,)),
            dma((n_z + 1,)),
            dma((n_y,)),
            dma((n_y,)),
            dma,
            dma,
            dma((4,)),
            dma((4,)),
            dma((14,)),
        ],
        compiler_params=pltpu.CompilerParams(
            collective_id=0, has_side_effects=True, vmem_limit_bytes=VMEM_BYTES
        ),
        name="layer",
    )(
        sink_logits,
        routes.T,
        route_weights.T,
        expert_input,
        norm_gain[None, :],
        queries,
        key_heads,
        value_heads,
        tables,
        gate_weight,
        up_weight,
        down_weight,
        mix_weight,
    )
    return pl.pallas_call(
        hand_over,
        in_specs=[vmem] * 2,
        out_specs=[anywhere] * 2,
        out_shape=shapes,
        scratch_shapes=[dma((2,))],
        name="hand_over",
    )(
        pltpu.with_memory_space_constraint(mixed, pltpu.VMEM),
        pltpu.with_memory_space_constraint(expert, pltpu.VMEM),
    )


def count_of(mesh, axis, among):
    coords = {getattr(d, "coords", (0, 0, 0))[axis] for d in mesh.devices.flat}
    return len(coords) if among % len(coords) == 0 else 1


def solution(mesh):
    n_ep, n_tp = mesh.shape["ep"], mesh.shape["tp"]
    n_z, n_y = count_of(mesh, 2, n_ep), count_of(mesh, 1, n_tp)
    n_z = n_z if n_z in (1, 2, 4) else 1
    grid = Mesh(mesh.devices.reshape(n_z, n_ep // n_z, n_tp), ("zz", "xx", "tp"))
    ep = ("zz", "xx")
    every = ("zz", "xx", "tp")
    return jax.shard_map(
        functools.partial(body, n_y),
        mesh=grid,
        in_specs=(
            P(ep, "tp"),
            P(ep, "tp"),
            P(ep, "tp"),
            P("tp"),
            P(),
            P(every, None),
            P(),
            P(every, None),
            P(every, None),
            P(every, None, None),
            P(every, None, None),
            P(every, None, None),
        ),
        out_specs=(P(every, None), P(every, None)),
        check_vma=False,
    )
```

```python
import functools

import jax
import jax.numpy as jnp
import numpy as np
from jax import lax
from jax.experimental import pallas as pl
from jax.experimental.pallas import tpu as pltpu
from jax.sharding import Mesh
from jax.sharding import PartitionSpec as P

HEAD_DIM = 64
WINDOW = 128
GRID_W = 64
ROPE_BASE = 10000.0
CLAMP_LIMIT = 7.0
GATE_SLOPE = 1.702
NORM_EPS = 1e-05

F32 = jnp.float32
BF16 = jnp.bfloat16
MESH = pl.DeviceIdType.MESH
PANELS = 2
TILE = 256
RELAYED = 256
VMEM_BYTES = 61 << 20

scope = jax.named_scope


def table_rows(rows_here):
    return -(-(rows_here + 2 * WINDOW) // GRID_W // 8) * 8


def angle_tables(length, rows_here):
    half = HEAD_DIM // 2
    quarter = HEAD_DIM // 4
    lane = np.arange(2 * HEAD_DIM) % HEAD_DIM
    freqs = (ROPE_BASE ** (-np.arange(0, half, 2) / half)).astype(np.float32)
    lane_freq = np.tile(freqs, 2 * HEAD_DIM // quarter)
    count = (length - rows_here) // GRID_W + table_rows(rows_here)
    by_row = np.arange(count) - WINDOW // GRID_W
    by_col = np.arange(WINDOW) % GRID_W
    place = np.concatenate([by_row, by_col]).astype(np.float32)
    angle = (place[:, None] * lane_freq[None, :]).astype(np.float64)
    sign = np.where(lane % half < quarter, -1.0, 1.0)
    return np.stack([np.cos(angle), np.sin(angle) * sign]).astype(np.float32)


def turn(cells, cosines, sines):
    quarter = HEAD_DIM // 4
    width = cells.shape[1]
    lane = lax.broadcasted_iota(jnp.int32, cells.shape, 1)
    ahead = pltpu.roll(cells, width - quarter, 1)
    behind = pltpu.roll(cells, quarter, 1)
    partner = jnp.where(lane % (2 * quarter) < quarter, ahead, behind)
    return cells * cosines + partner * sines

def kernel(
    sizes,
    sink_hbm,
    route_hbm,
    share_hbm,
    x_hbm,
    gain_hbm,
    q_hbm,
    k_hbm,
    v_hbm,
    table_hbm,
    wg_hbm,
    wu_hbm,
    wd_hbm,
    mix_hbm,
    mixer_ref,
    expert_ref,
    sink,
    route_ref,
    share_ref,
    x_ref,
    gain_ref,
    q_ref,
    k_ref,
    v_ref,
    by_row,
    by_col,
    k_scr,
    v_scr,
    halo,
    att,
    att_in,
    routing,
    normed,
    picks,
    outgoing,
    arrived,
    produced,
    returned,
    shares,
    partial,
    home,
    relayed,
    relay_shares,
    relay_sum,
    relay_home,
    crossed,
    wg,
    wu,
    wd,
    mix,
    act,
    z_send,
    z_recv,
    rt_send,
    rt_recv,
    out_send,
    out_recv,
    back_send,
    back_recv,
    home_send,
    home_recv,
    relay_send,
    relay_recv,
    sum_send,
    sum_recv,
    cross_send,
    cross_recv,
    att_send,
    att_recv,
    halo_send,
    halo_recv,
    load_sem,
):
    n_z, n_x, n_y, n_tp, top_count, capacity = sizes
    n_ep = n_z * n_x
    plane = n_x * n_tp
    slots = plane * capacity
    cores = n_tp // n_y
    side = n_x * cores
    z, x, t = lax.axis_index("zz"), lax.axis_index("xx"), lax.axis_index("tp")
    me = x * n_tp + t
    y, core = lax.div(t, cores), lax.rem(t, cores)
    ep = z * n_x + x
    rows_here, width_q = q_ref.shape
    tok, width = x_ref.shape
    panel = width // PANELS
    back_width = [panel] * (PANELS - 1) + [panel - RELAYED]
    relay_cols = pl.ds(panel - RELAYED, RELAYED)
    length = rows_here * n_ep
    kv_local = k_scr.shape[0]
    bq = WINDOW
    span = bq + 2 * WINDOW
    blocks = rows_here // bq
    chunk = rows_here // n_tp
    last = n_z - 1
    grid_rows = by_row.shape[1]
    table_end = table_hbm.shape[1] - WINDOW

    def z_dev(b):
        return (b, x, t)

    def plane_dev(p):
        return (z, lax.div(p, n_tp), lax.rem(p, n_tp))

    def ep_dev(e):
        return (lax.div(e, n_x), lax.rem(e, n_x), t)

    after, before = lax.rem(ep + 1, n_ep), lax.rem(ep + n_ep - 1, n_ep)
    has_after, has_before = ep < n_ep - 1, ep > 0
    has_up, has_down = z < last, z > 0
    end = (z == 0) | (z == last)
    mid = (z > 0) & (z < last)

    closer = jnp.minimum(z, last - z)
    far_side = jnp.where(z < last - z, 1, -1)

    def nearest(i):
        if i == 0:
            return z
        paired = z + ((i + 1) // 2) * (-1 if i % 2 else 1)
        return jnp.where(i <= 2 * closer, paired, z + far_side * (i - closer))

    def going_back(i):
        return lax.bitwise_xor(z, jnp.int32(last - i))

    first_row = pl.multiple_of(ep * (rows_here // GRID_W), 8)
    loads = {
        "route": (route_hbm, route_ref),
        "share": (share_hbm, share_ref),
        "x": (x_hbm, x_ref),
        "gain": (gain_hbm, gain_ref),
        "sink": (sink_hbm, sink),
        "k": (k_hbm, k_ref),
        "v": (v_hbm, v_ref),
        "by_row": (table_hbm.at[:, pl.ds(first_row, grid_rows)], by_row),
        "by_col": (table_hbm.at[:, pl.ds(table_end, WINDOW)], by_col),
        "q": (q_hbm, q_ref),
        "wg": (wg_hbm.at[0], wg),
        "wu": (wu_hbm.at[0], wu),
        "wd": (wd_hbm.at[0], wd),
        "mix": (mix_hbm, mix),
    }
    loads = {
        name: pltpu.make_async_copy(source, target, load_sem.at[i])
        for i, (name, (source, target)) in enumerate(loads.items())
    }
    for load in loads.values():
        load.start()

    def loaded(*names):
        for name in names:
            loads[name].wait()

    barrier = pltpu.get_barrier_semaphore()

    def greet_z(o, _):
        pl.semaphore_signal(barrier, inc=1, device_id=z_dev(lax.rem(z + o, n_z)), device_id_type=MESH)
        return 0

    def greet_plane(p, _):
        pl.semaphore_signal(
            barrier, inc=1, device_id=plane_dev(lax.rem(me + p, plane)), device_id_type=MESH
        )
        return 0

    def column(o):
        b, row = lax.rem(z + o // n_y, n_z), lax.rem(y + o % n_y, n_y)
        return (b, x, row * cores + core)

    lax.fori_loop(1, n_z, greet_z, 0)
    for o in range(n_y + 1, n_z * n_y):
        if o % n_y:
            pl.semaphore_signal(barrier, inc=1, device_id=column(o), device_id_type=MESH)
    lax.fori_loop(1, plane, greet_plane, 0)
    for e in (after, before):
        pl.semaphore_signal(barrier, inc=1, device_id=ep_dev(e), device_id_type=MESH)

    def await_bytes(ref, sem):
        pltpu.make_async_copy(ref, ref, sem).wait()

    upper = (
        lax.broadcasted_iota(jnp.int32, (tok, tok), 0) < lax.broadcasted_iota(jnp.int32, (tok, tok), 1)
    ).astype(F32).astype(BF16)

    def pick_rows(route, expert_of_slot, count):
        slot_row = lax.broadcasted_iota(jnp.int32, (count, tok), 0)
        lane_expert = expert_of_slot(lax.div(slot_row, capacity)).astype(F32)
        place_in = lax.rem(slot_row, capacity).astype(F32)
        member = jnp.zeros((count, tok), F32)
        share = jnp.zeros((count, tok), F32)
        for k in range(top_count):
            hit = route[k : k + 1, :] == lane_expert
            member = jnp.where(hit, 1.0, member)
            share = jnp.where(hit, route[top_count + k : top_count + k + 1, :], share)
        rank = jnp.dot(member.astype(BF16), upper, preferred_element_type=F32)
        pick = jnp.where(rank == place_in, member, 0.0)
        scaled = (share * pick).T
        coarse = scaled.astype(BF16)
        return pick, coarse, (scaled - coarse.astype(F32)).astype(BF16)

    def choose(i):
        b = nearest(i)
        if i > 0:
            await_bytes(routing.at[b, y], rt_recv.at[b, y])
        pick, coarse, fine = pick_rows(routing[b, y], lambda e: z * plane + e, slots)
        picks[...] = pick.astype(BF16)
        shares[b, 0] = coarse
        shares[b, 1] = fine

    def choose_relayed(i):
        b = nearest(i)

        def expert(e):
            return z * plane + lax.div(e, cores) * n_tp + y * cores + lax.rem(e, cores)

        for o in range(n_y):
            row = lax.rem(y + o, n_y)
            if o > 0:
                await_bytes(routing.at[b, row], rt_recv.at[b, row])
            _, coarse, fine = pick_rows(routing[b, row], expert, side * capacity)
            relay_shares[b, row, 0] = coarse
            relay_shares[b, row, 1] = fine

    loaded("route", "share")
    routing[z, y, :top_count, :] = route_ref[...].astype(F32)
    routing[z, y, top_count:, :] = share_ref[...]
    choose(0)
    loaded("x", "gain")
    with scope("norm"):
        for part in range(tok // 32):
            rows = slice(part * 32, part * 32 + 32)
            values = x_ref[rows, :].astype(F32)
            center = jnp.mean(values, axis=1, keepdims=True)
            spread = jnp.mean(jnp.square(values - center), axis=1, keepdims=True)
            result = ((values - center) * lax.rsqrt(spread + NORM_EPS) * gain_ref[...]).astype(BF16)
            for h in range(PANELS):
                normed[z, h, rows, :] = result[:, h * panel : h * panel + panel]
    with scope("barr"):
        pl.semaphore_wait(barrier, (n_z - 1) * n_y + plane - 1 + 2)

    def rt_copy(o):
        return pltpu.make_async_remote_copy(
            src_ref=routing.at[z, y],
            dst_ref=routing.at[z, y],
            send_sem=rt_send.at[o],
            recv_sem=rt_recv.at[z, y],
            device_id=column(o),
            device_id_type=MESH,
        )

    def z_copy(i, h, b, target):
        return pltpu.make_async_remote_copy(
            src_ref=normed.at[b, h],
            dst_ref=normed.at[b, h],
            send_sem=z_send.at[i, h],
            recv_sem=z_recv.at[b, h],
            device_id=z_dev(target),
            device_id_type=MESH,
        )

    def onward(i):
        b = nearest(i)
        target = jnp.where(b < z, z + 1, z - 1)
        return b, target, (target >= 0) & (target <= last)

    for o in range(1, n_z * n_y):
        rt_copy(o).start()
    if n_z > 1:
        for h in range(PANELS):

            @pl.when(has_up)
            def _():
                z_copy(0, h, z, z + 1).start()

            @pl.when(has_down)
            def _():
                z_copy(n_z, h, z, z - 1).start()

    def tick(distance, h):
        for i in range(1, n_z):
            if not (i + 1) // 2 <= distance <= i:
                continue
            b, target, goes_on = onward(i)

            @pl.when(jnp.abs(b - z) == distance)
            def _():
                with scope(f"zwait{i}{h}"):
                    await_bytes(normed.at[b, h], z_recv.at[b, h])

                @pl.when(goes_on)
                def _():
                    z_copy(i, h, b, target).start()

    def dispatch(i, h):
        b = nearest(i)
        with scope(f"disp{i}{h}"):
            if h == 0 and i > 0:
                choose(i)

            def tile(j, _):
                cols = pl.ds(pl.multiple_of(j * TILE, TILE), TILE)
                outgoing[b, h, :, cols] = jnp.dot(
                    picks[...], normed[b, h, :, cols], preferred_element_type=F32
                ).astype(BF16)
                return 0

            parts = 2 if i == 0 and h == 0 else 1
            each = panel // parts
            for part in range(parts):
                lax.fori_loop(part * each // TILE, (part + 1) * each // TILE, tile, 0)
                exchange(outgoing, arrived, out_send, out_recv, b, h, each, part * each)

    def exchange(source, target, send, recv, b, h, count, at=0):
        mine = pl.ds(pl.multiple_of(me * capacity, capacity), capacity)
        cols = pl.ds(at, count)

        def one(p, _):
            to = lax.rem(me + p, plane)
            pltpu.make_async_remote_copy(
                src_ref=source.at[b, h, pl.ds(pl.multiple_of(to * capacity, capacity), capacity), cols],
                dst_ref=target.at[b, h, mine, cols],
                send_sem=send.at[b, h],
                recv_sem=recv.at[b, h],
                device_id=plane_dev(to),
                device_id_type=MESH,
            ).start()
            return 0

        lax.fori_loop(1, plane, one, 0)
        pltpu.make_async_copy(
            source.at[b, h, mine, cols], target.at[b, h, mine, cols], recv.at[b, h]
        ).start()

    def halo_copy(source, which, start, target):
        return pltpu.make_async_remote_copy(
            src_ref=source.at[pl.ds(start, WINDOW)],
            dst_ref=halo.at[which],
            send_sem=halo_send.at[which],
            recv_sem=halo_recv.at[which],
            device_id=ep_dev(target),
            device_id_type=MESH,
        )

    to_after = [
        halo_copy(k_ref, 0, rows_here - WINDOW, after),
        halo_copy(v_ref, 1, rows_here - WINDOW, after),
    ]
    to_before = [halo_copy(k_ref, 2, 0, before), halo_copy(v_ref, 3, 0, before)]

    def send_halos():
        for there, copies in ((has_after, to_after), (has_before, to_before)):

            @pl.when(there)
            def _():
                for copy in copies:
                    copy.start()

    def await_halos():
        for there, copies in ((has_before, to_after), (has_after, to_before)):

            @pl.when(there)
            def _():
                for copy in copies:
                    copy.wait_recv()

        for there, which in ((has_before, 0), (has_after, 2)):

            @pl.when(jnp.logical_not(there))
            def _():
                halo[which] = jnp.zeros(halo.shape[1:], BF16)
                halo[which + 1] = jnp.zeros(halo.shape[1:], BF16)

    of_row = lax.rem(lax.broadcasted_iota(jnp.int32, (WINDOW, 128), 1), HEAD_DIM) < HEAD_DIM // 2

    def angles(which, at):
        start = lax.div(at, GRID_W)
        parts = [
            jnp.broadcast_to(by_row[which, pl.ds(start + i, 1), :], (GRID_W, 128))
            for i in range(WINDOW // GRID_W)
        ]
        return jnp.where(of_row, jnp.concatenate(parts, axis=0), by_col[which])

    def place(source, values, at, count):
        cosines, sines = angles(0, at), angles(1, at)
        for pair in range(kv_local // 2):
            cols = slice(pair * 128, pair * 128 + 128)
            turned = turn(source[:, cols].astype(F32), cosines, sines).astype(BF16)
            piece = values[:, cols]
            for side in range(2):
                lanes = slice(side * 64, side * 64 + 64)
                k_scr[2 * pair + side, pl.ds(at, count), :] = turned[:, lanes]
                v_scr[2 * pair + side, pl.ds(at, count), :] = piece[:, lanes]

    def place_own(i, _):
        at = pl.multiple_of(i * 128, 128)
        place(k_ref[pl.ds(at, 128), :], v_ref[pl.ds(at, 128), :], WINDOW + at, 128)
        return 0

    row = lax.rem(lax.broadcasted_iota(jnp.int32, (2 * bq, span), 0), bq)
    col = lax.broadcasted_iota(jnp.int32, (2 * bq, span), 1)
    top = lax.broadcasted_iota(jnp.int32, (2 * bq, 1), 0) < bq

    def attend(block, _):
        first = pl.multiple_of(block * bq, bq)
        cosines = angles(0, first + WINDOW) * HEAD_DIM**-0.5
        sines = angles(1, first + WINDOW) * HEAD_DIM**-0.5
        key_pos = ep * rows_here + first - WINDOW + col
        inside = (col >= row) & (col <= row + 2 * WINDOW) & (key_pos >= 0) & (key_pos < length)
        for g in range(kv_local):
            q = q_ref[pl.ds(first, bq), g * 128 : g * 128 + 128].astype(F32)
            q = turn(q, cosines, sines).astype(BF16)
            q2 = jnp.concatenate([q[:, :64], q[:, 64:]], axis=0)
            k = k_scr[g, pl.ds(first, span), :]
            v = v_scr[g, pl.ds(first, span), :]
            scores = lax.dot_general(q2, k, (((1,), (1,)), ((), ())), preferred_element_type=F32)
            scores = jnp.where(inside, scores, -jnp.inf)
            logit = jnp.where(top, sink[2 * g], sink[2 * g + 1])
            peak = jnp.maximum(jnp.max(scores, axis=1, keepdims=True), logit)
            weights = jnp.exp(scores - peak)
            total = jnp.sum(weights, axis=1, keepdims=True) + jnp.exp(logit - peak)
            chances = (weights * (1.0 / total)).astype(BF16)
            blend = jnp.dot(chances, v, preferred_element_type=F32).astype(BF16)
            att[pl.ds(first, bq), g * 128 : g * 128 + 128] = jnp.concatenate(
                [blend[:bq], blend[bq:]], axis=1
            )
        return 0

    def attend_inner(part, parts):
        inner = blocks - 2
        with scope(f"att{part}"):
            lax.fori_loop(1 + inner * part // parts, 1 + inner * (part + 1) // parts, attend, 0)

    def attend_edges():
        with scope("halowait"):
            await_halos()
        with scope("edges"):
            place(halo[0], halo[1], 0, WINDOW)
            place(halo[2], halo[3], WINDOW + rows_here, WINDOW)
            lax.fori_loop(0, 2, lambda i, _: attend(i * (blocks - 1), _), 0)

    def send_heads(edges):
        each = chunk // bq

        def one(p, _):
            to = lax.rem(t + p, n_tp)
            for i in range(each):
                block = to * each + i
                at_edge = (block == 0) | (block == blocks - 1)

                @pl.when(at_edge if edges else jnp.logical_not(at_edge))
                def _():
                    pltpu.make_async_remote_copy(
                        src_ref=att.at[pl.ds(pl.multiple_of(block * bq, bq), bq)],
                        dst_ref=att_in.at[t, i * bq : i * bq + bq],
                        send_sem=att_send,
                        recv_sem=att_recv,
                        device_id=(z, x, to),
                        device_id_type=MESH,
                    ).start()

            return 0

        lax.fori_loop(1, n_tp, one, 0)
        if edges:
            own = pl.ds(pl.multiple_of(t * chunk, chunk), chunk)
            pltpu.make_async_copy(att.at[own], att_in.at[t], att_recv).start()

    def mixer():
        with scope("attwait"):
            await_bytes(att_in, att_recv)
        loaded("mix")

        def tile(j, _):
            cols = pl.ds(pl.multiple_of(j * TILE, TILE), TILE)
            total = jnp.zeros((chunk, TILE), F32)
            for s in range(n_tp):
                total = total + jnp.dot(
                    att_in[s], mix[s * width_q : s * width_q + width_q, cols], preferred_element_type=F32
                )
            mixer_ref[:, cols] = total.astype(BF16)
            return 0

        with scope("mixer"):
            lax.fori_loop(0, width // TILE, tile, 0)

    def experts(i, sent=lambda h: None):
        b = nearest(i)
        hidden = wg.shape[1]
        for h in range(PANELS):
            with scope(f"arrwait{i}{h}"):
                await_bytes(arrived.at[b, h], out_recv.at[b, h])

        def up(j, _):
            cols = pl.ds(pl.multiple_of(j * TILE, TILE), TILE)
            gate = jnp.zeros((slots, TILE), F32)
            lift = jnp.zeros((slots, TILE), F32)
            for h in range(PANELS):
                rows = arrived[b, h]
                deep = slice(h * panel, h * panel + panel)
                gate = gate + jnp.dot(rows, wg[deep, cols], preferred_element_type=F32)
                lift = lift + jnp.dot(rows, wu[deep, cols], preferred_element_type=F32)
            gate = jnp.minimum(gate, CLAMP_LIMIT)
            lift = jnp.clip(lift, -CLAMP_LIMIT, CLAMP_LIMIT)
            act[:, cols] = ((lift + 1.0) * gate * jax.nn.sigmoid(GATE_SLOPE * gate)).astype(BF16)
            return 0

        with scope(f"exp{i}"):
            lax.fori_loop(0, hidden // TILE, up, 0)
            for h in range(PANELS):

                def down(j, _):
                    cols = pl.ds(pl.multiple_of(j * TILE, TILE), TILE)
                    wide = pl.ds(pl.multiple_of(h * panel + j * TILE, TILE), TILE)
                    produced[b, h, :, cols] = jnp.dot(
                        act[...], wd[:, wide], preferred_element_type=F32
                    ).astype(BF16)
                    return 0

                lax.fori_loop(0, panel // TILE, down, 0)
                sent(h)

    def send_back(b, h):
        exchange(produced, returned, back_send, back_recv, b, h, back_width[h])

    def send_relayed(b):
        mine = pl.ds(pl.multiple_of((x * cores + core) * capacity, capacity), capacity)

        def source(to, row):
            slot = lax.div(to, cores) * n_tp + row * cores + lax.rem(to, cores)
            rows = pl.ds(pl.multiple_of(slot * capacity, capacity), capacity)
            return produced.at[b, PANELS - 1, rows, relay_cols]

        def one(p, _):
            to = lax.rem(x * cores + core + p, side)
            for row in range(n_y):
                pltpu.make_async_remote_copy(
                    src_ref=source(to, row),
                    dst_ref=relayed.at[b, row, mine],
                    send_sem=relay_send.at[b],
                    recv_sem=relay_recv.at[b],
                    device_id=(z, lax.div(to, cores), y * cores + lax.rem(to, cores)),
                    device_id_type=MESH,
                ).start()
            return 0

        lax.fori_loop(1, side, one, 0)
        for row in range(n_y):
            pltpu.make_async_copy(
                source(x * cores + core, row), relayed.at[b, row, mine], relay_recv.at[b]
            ).start()

    def homeward(b):
        target = jnp.where(b < z, z - 1, z + 1)
        return target, jnp.where((target == b) & (b < z), n_z, b)

    def home_copy(b, h):
        target, slot = homeward(b)
        cols = pl.ds(0, back_width[h])
        return pltpu.make_async_remote_copy(
            src_ref=partial.at[b, h, :, cols],
            dst_ref=home.at[slot, h, :, cols],
            send_sem=home_send.at[b, h],
            recv_sem=home_recv.at[slot, h],
            device_id=z_dev(target),
            device_id_type=MESH,
        )

    def relay_copy(b):
        target, slot = homeward(b)
        return pltpu.make_async_remote_copy(
            src_ref=relay_sum.at[b],
            dst_ref=relay_home.at[slot],
            send_sem=sum_send.at[b],
            recv_sem=sum_recv.at[slot],
            device_id=z_dev(target),
            device_id_type=MESH,
        )

    def cross_copy(o):
        row = lax.rem(y + o, n_y)
        return pltpu.make_async_remote_copy(
            src_ref=relay_sum.at[z, row],
            dst_ref=crossed.at[y],
            send_sem=cross_send.at[o],
            recv_sem=cross_recv.at[y],
            device_id=(z, x, row * cores + core),
            device_id_type=MESH,
        )

    def clear_home():
        for slot, missing in ((z, z == 0), (n_z, z == last)):

            @pl.when(missing)
            def _():
                home[slot] = jnp.zeros(home.shape[1:], BF16)
                relay_home[slot] = jnp.zeros(relay_home.shape[1:], BF16)

    def weighted(b, h, cols):
        rows = returned[b, h, :, cols]
        total = jnp.dot(shares[b, 0], rows, preferred_element_type=F32)
        return total + jnp.dot(shares[b, 1], rows, preferred_element_type=F32)

    def relay_weighted(b, row):
        rows = relayed[b, row]
        total = jnp.dot(relay_shares[b, row, 0], rows, preferred_element_type=F32)
        return total + jnp.dot(relay_shares[b, row, 1], rows, preferred_element_type=F32)

    def combine_relayed(name, b, further):
        with scope(f"relwait{name}"):
            await_bytes(relayed.at[b], relay_recv.at[b])
            if further:
                await_bytes(relay_home.at[b], sum_recv.at[b])

        with scope(f"rel{name}"):
            for row in range(n_y):
                total = relay_weighted(b, row)
                if further:
                    total = total + relay_home[b, row].astype(F32)
                relay_sum[b, row] = total.astype(BF16)
        relay_copy(b).start()

    def from_both_sides(place, sem):
        @pl.when(has_down)
        def _():
            await_bytes(place(z), sem(z))

        @pl.when(has_up)
        def _():
            await_bytes(place(n_z), sem(n_z))

    def combine_own_relayed():
        with scope("relwaitown"):
            await_bytes(relayed.at[z], relay_recv.at[z])
            from_both_sides(lambda slot: relay_home.at[slot], lambda slot: sum_recv.at[slot])
        for row in range(n_y):
            total = relay_weighted(z, row) + relay_home[z, row].astype(F32)
            relay_sum[z, row] = (total + relay_home[n_z, row].astype(F32)).astype(BF16)
        for o in range(1, n_y):
            cross_copy(o).start()

    def finish_relayed():
        total = relay_sum[z, y].astype(F32)
        for o in range(1, n_y):
            row = lax.rem(y + o, n_y)
            with scope("crosswait"):
                await_bytes(crossed.at[row], cross_recv.at[row])
            total = total + crossed[row].astype(F32)
        expert_ref[:, width - RELAYED :] = total.astype(BF16)

    def combine(name, b, h, further):
        cols = pl.ds(0, back_width[h])
        with scope(f"retwait{name}"):
            await_bytes(returned.at[b, h, :, cols], back_recv.at[b, h])

        if further:
            with scope(f"chain{name}"):
                await_bytes(home.at[b, h, :, cols], home_recv.at[b, h])

        def tile(j, _):
            cols = pl.ds(pl.multiple_of(j * TILE, TILE), TILE)
            total = weighted(b, h, cols)
            if further:
                total = total + home[b, h, :, cols].astype(F32)
            partial[b, h, :, cols] = total.astype(BF16)
            return 0

        with scope(f"comb{name}"):
            lax.fori_loop(0, back_width[h] // TILE, tile, 0)
        home_copy(b, h).start()

    def combine_own(h):
        here = pl.ds(0, back_width[h])
        with scope(f"retwaitown{h}"):
            await_bytes(returned.at[z, h, :, here], back_recv.at[z, h])
        with scope(f"homewait{h}"):
            from_both_sides(lambda slot: home.at[slot, h, :, here], lambda slot: home_recv.at[slot, h])

        def tile(j, _):
            cols = pl.ds(pl.multiple_of(j * TILE, TILE), TILE)
            wide = pl.ds(pl.multiple_of(h * panel + j * TILE, TILE), TILE)
            total = weighted(z, h, cols) + home[z, h, :, cols].astype(F32)
            total = total + home[n_z, h, :, cols].astype(F32)
            expert_ref[:, wide] = total.astype(BF16)
            return 0

        with scope(f"combown{h}"):
            lax.fori_loop(0, back_width[h] // TILE, tile, 0)

    for h in range(PANELS):
        dispatch(0, h)
    clear_home()
    loaded("k", "v", "by_row", "by_col", "q", "sink")
    with scope("place"):
        lax.fori_loop(0, rows_here // 128, place_own, 0)
    attend_inner(0, 3)
    for h in range(PANELS):
        if n_z > 1:
            tick(1, h)
            dispatch(1, h)
        attend_inner(1 + h, 3)
    if n_z > 2:
        tick(2, 0)
        dispatch(2, 0)
    loaded("wg", "wu", "wd")
    if n_z > 1:
        experts(0)
    if n_z > 2:
        tick(2, 1)
        dispatch(2, 1)
        experts(1)
        for h in range(PANELS):
            tick(3, h)
            dispatch(3, h)
    send_halos()
    send_heads(False)
    if n_z > 1:
        send_relayed(z)
    if n_z > 2:
        send_relayed(nearest(1))
    with scope("chooserel"):
        for i in range(n_z):
            choose_relayed(i)
    if n_z > 2:
        experts(2)
        send_relayed(nearest(2))

        @pl.when(mid)
        def _():
            for h in range(PANELS):
                send_back(going_back(0), h)

    def sent(h):
        if h == PANELS - 1:
            send_relayed(nearest(last))

        @pl.when(end)
        def _():
            send_back(going_back(0), h)

    def sums(steps, further=False):
        for i, h in steps:
            if h is None:
                combine_relayed(i, going_back(i), further)
            else:
                combine(f"{i}{h}", going_back(i), h, further)

    def all_of(i):
        return [(i, h) for h in range(PANELS)]

    experts(last, sent)
    if n_z > 2:

        @pl.when(end)
        def _():
            sums([(2, None), (1, None)])

    attend_edges()
    send_heads(True)
    for i in range(1, n_z):
        for h in range(PANELS if i < last else PANELS - 1):
            send_back(going_back(i), h)
    if n_z > 2:

        @pl.when(end)
        def _():
            sums([(0, None)] + all_of(0))
            mixer()
            sums(all_of(1))

        @pl.when(mid)
        def _():
            sums([(0, None), (1, None)], True)
            mixer()
            sums([(2, None)] + all_of(1), True)
    else:
        if n_z > 1:
            sums([(0, None)] + all_of(0))
        mixer()
    combine_own_relayed()
    if n_z > 1:
        send_back(z, PANELS - 1)
    if n_z > 2:

        @pl.when(end)
        def _():
            sums(all_of(2))

        @pl.when(mid)
        def _():
            sums([(i, h) for h in range(PANELS) for i in (2, 0)], True)

    for o in range(1, n_z * n_y):
        rt_copy(o).wait_send()
    if n_z > 1:
        for h in range(PANELS):

            @pl.when(has_up)
            def _():
                z_copy(0, h, z, z + 1).wait_send()

            @pl.when(has_down)
            def _():
                z_copy(n_z, h, z, z - 1).wait_send()

            for i in range(1, n_z):
                b, target, goes_on = onward(i)

                @pl.when(goes_on)
                def _():
                    z_copy(i, h, b, target).wait_send()
    for there, copies in ((has_after, to_after), (has_before, to_before)):

        @pl.when(there)
        def _():
            for copy in copies:
                copy.wait_send()

    for b in range(n_z):
        for h in range(PANELS):
            gone = pl.ds(0, (plane - 1) * capacity)
            await_bytes(outgoing.at[b, h, gone], out_send.at[b, h])
        gone = pl.ds(0, (side - 1) * n_y * capacity)
        await_bytes(produced.at[b, 0, gone, pl.ds(0, RELAYED)], relay_send.at[b])
    await_bytes(att.at[pl.ds(0, (n_tp - 1) * chunk)], att_send)

    for h in range(PANELS):
        combine_own(h)
        if h == 0:
            finish_relayed()

    with scope("late"):
        for h in range(PANELS):
            for i in range(1, n_z):
                home_copy(nearest(i), h).wait_send()
            for b in range(n_z):
                gone = pl.ds(0, (plane - 1) * capacity)
                await_bytes(produced.at[b, h, gone, pl.ds(0, back_width[h])], back_send.at[b, h])
        for i in range(1, n_z):
            relay_copy(nearest(i)).wait_send()
        for o in range(1, n_y):
            cross_copy(o).wait_send()


def hand_over(mixer_in, expert_in, mixer_out, expert_out, sem):
    copies = [
        pltpu.make_async_copy(source, target, sem.at[i])
        for i, (source, target) in enumerate(((mixer_in, mixer_out), (expert_in, expert_out)))
    ]
    for copy in copies:
        copy.start()
    for copy in copies:
        copy.wait()


def body(
    n_y,
    queries,
    key_heads,
    value_heads,
    sink_logits,
    mix_weight,
    expert_input,
    norm_gain,
    routes,
    route_weights,
    gate_weight,
    up_weight,
    down_weight,
):
    n_z, n_x, n_tp = lax.axis_size("zz"), lax.axis_size("xx"), lax.axis_size("tp")
    n_ep = n_z * n_x
    plane = n_x * n_tp
    rows_here, width_q = queries.shape
    kv_width = key_heads.shape[1]
    kv_local = kv_width // HEAD_DIM
    tok, top_count = routes.shape
    capacity = 2 * tok * top_count // (n_ep * n_tp)
    slots = plane * capacity
    width = expert_input.shape[1]
    panel = width // PANELS
    hidden = gate_weight.shape[2]
    tables = jnp.asarray(angle_tables(rows_here * n_ep, rows_here))
    anywhere = pl.BlockSpec(memory_space=pl.ANY)
    vmem = pl.BlockSpec(memory_space=pltpu.VMEM)
    reach = rows_here + 2 * WINDOW
    dma = pltpu.SemaphoreType.DMA
    shapes = [
        jax.ShapeDtypeStruct((rows_here // n_tp, width), BF16),
        jax.ShapeDtypeStruct((tok, width), BF16),
    ]
    both = dma((n_z, PANELS))
    side_slots = slots // n_y
    mixed, expert = pl.pallas_call(
        functools.partial(kernel, (n_z, n_x, n_y, n_tp, top_count, capacity)),
        in_specs=[anywhere] * 13,
        out_specs=[vmem] * 2,
        out_shape=[pltpu.VMEM(s.shape, s.dtype) for s in shapes],
        scratch_shapes=[
            pltpu.SMEM(sink_logits.shape, F32),
            pltpu.VMEM((top_count, tok), jnp.int32),
            pltpu.VMEM((top_count, tok), F32),
            pltpu.VMEM((tok, width), BF16),
            pltpu.VMEM((1, width), F32),
            pltpu.VMEM((rows_here, width_q), BF16),
            pltpu.VMEM((rows_here, kv_width), BF16),
            pltpu.VMEM((rows_here, kv_width), BF16),
            pltpu.VMEM((2, table_rows(rows_here), 128), F32),
            pltpu.VMEM((2, WINDOW, 128), F32),
            pltpu.VMEM((kv_local, reach, HEAD_DIM), BF16),
            pltpu.VMEM((kv_local, reach, HEAD_DIM), BF16),
            pltpu.VMEM((4, WINDOW, kv_width), BF16),
            pltpu.VMEM((rows_here, width_q), BF16),
            pltpu.VMEM((n_tp, rows_here // n_tp, width_q), BF16),
            pltpu.VMEM((n_z, n_y, 2 * top_count, tok), F32),
            pltpu.VMEM((n_z, PANELS, tok, panel), BF16),
            pltpu.VMEM((slots, tok), BF16),
            pltpu.VMEM((n_z, PANELS, slots, panel), BF16),
            pltpu.VMEM((n_z, PANELS, slots, panel), BF16),
            pltpu.VMEM((n_z, PANELS, slots, panel), BF16),
            pltpu.VMEM((n_z, PANELS, slots, panel), BF16),
            pltpu.VMEM((n_z, 2, tok, slots), BF16),
            pltpu.VMEM((n_z, PANELS, tok, panel), BF16),
            pltpu.VMEM((n_z + 1, PANELS, tok, panel), BF16),
            pltpu.VMEM((n_z, n_y, side_slots, RELAYED), BF16),
            pltpu.VMEM((n_z, n_y, 2, tok, side_slots), BF16),
            pltpu.VMEM((n_z, n_y, tok, RELAYED), BF16),
            pltpu.VMEM((n_z + 1, n_y, tok, RELAYED), BF16),
            pltpu.VMEM((n_y, tok, RELAYED), BF16),
            pltpu.VMEM((width, hidden), BF16),
            pltpu.VMEM((width, hidden), BF16),
            pltpu.VMEM((hidden, width), BF16),
            pltpu.VMEM(mix_weight.shape, BF16),
            pltpu.VMEM((slots, hidden), BF16),
            dma((n_z + 1, PANELS)),
            both,
            dma((n_z * n_y,)),
            dma((n_z, n_y)),
            both,
            both,
            both,
            both,
            both,
            dma((n_z + 1, PANELS)),
            dma((n_z,)),
            dma((n_z,)),
            dma((n_z,)),
            dma((n_z + 1,)),
            dma((n_y,)),
            dma((n_y,)),
            dma,
            dma,
            dma((4,)),
            dma((4,)),
            dma((14,)),
        ],
        compiler_params=pltpu.CompilerParams(
            collective_id=0, has_side_effects=True, vmem_limit_bytes=VMEM_BYTES
        ),
        name="layer",
    )(
        sink_logits,
        routes.T,
        route_weights.T,
        expert_input,
        norm_gain[None, :],
        queries,
        key_heads,
        value_heads,
        tables,
        gate_weight,
        up_weight,
        down_weight,
        mix_weight,
    )
    return pl.pallas_call(
        hand_over,
        in_specs=[vmem] * 2,
        out_specs=[anywhere] * 2,
        out_shape=shapes,
        scratch_shapes=[dma((2,))],
        name="hand_over",
    )(
        pltpu.with_memory_space_constraint(mixed, pltpu.VMEM),
        pltpu.with_memory_space_constraint(expert, pltpu.VMEM),
    )


def count_of(mesh, axis, among):
    coords = {getattr(d, "coords", (0, 0, 0))[axis] for d in mesh.devices.flat}
    return len(coords) if among % len(coords) == 0 else 1


def solution(mesh):
    n_ep, n_tp = mesh.shape["ep"], mesh.shape["tp"]
    n_z, n_y = count_of(mesh, 2, n_ep), count_of(mesh, 1, n_tp)
    n_z = n_z if n_z in (1, 2, 4) else 1
    grid = Mesh(mesh.devices.reshape(n_z, n_ep // n_z, n_tp), ("zz", "xx", "tp"))
    ep = ("zz", "xx")
    every = ("zz", "xx", "tp")
    return jax.shard_map(
        functools.partial(body, n_y),
        mesh=grid,
        in_specs=(
            P(ep, "tp"),
            P(ep, "tp"),
            P(ep, "tp"),
            P("tp"),
            P(),
            P(every, None),
            P(),
            P(every, None),
            P(every, None),
            P(every, None, None),
            P(every, None, None),
            P(every, None, None),
        ),
        out_specs=(P(every, None), P(every, None)),
        check_vma=False,
    )
```

```python
import functools

import jax
import jax.numpy as jnp
import numpy as np
from jax import lax
from jax.experimental import pallas as pl
from jax.experimental.pallas import tpu as pltpu
from jax.sharding import Mesh
from jax.sharding import PartitionSpec as P

HEAD_DIM = 64
WINDOW = 128
GRID_W = 64
ROPE_BASE = 10000.0
CLAMP_LIMIT = 7.0
GATE_SLOPE = 1.702
NORM_EPS = 1e-05

F32 = jnp.float32
BF16 = jnp.bfloat16
MESH = pl.DeviceIdType.MESH
PANELS = 2
TILE = 256
RELAYED = 256
VMEM_BYTES = 61 << 20

scope = jax.named_scope


def table_rows(rows_here):
    return -(-(rows_here + 2 * WINDOW) // GRID_W // 8) * 8


def angle_tables(length, rows_here):
    half = HEAD_DIM // 2
    quarter = HEAD_DIM // 4
    lane = np.arange(2 * HEAD_DIM) % HEAD_DIM
    freqs = (ROPE_BASE ** (-np.arange(0, half, 2) / half)).astype(np.float32)
    lane_freq = np.tile(freqs, 2 * HEAD_DIM // quarter)
    count = (length - rows_here) // GRID_W + table_rows(rows_here)
    by_row = np.arange(count) - WINDOW // GRID_W
    by_col = np.arange(WINDOW) % GRID_W
    place = np.concatenate([by_row, by_col]).astype(np.float32)
    angle = (place[:, None] * lane_freq[None, :]).astype(np.float64)
    sign = np.where(lane % half < quarter, -1.0, 1.0)
    return np.stack([np.cos(angle), np.sin(angle) * sign]).astype(np.float32)


def turn(cells, cosines, sines):
    quarter = HEAD_DIM // 4
    width = cells.shape[1]
    lane = lax.broadcasted_iota(jnp.int32, cells.shape, 1)
    ahead = pltpu.roll(cells, width - quarter, 1)
    behind = pltpu.roll(cells, quarter, 1)
    partner = jnp.where(lane % (2 * quarter) < quarter, ahead, behind)
    return cells * cosines + partner * sines

def kernel(
    sizes,
    sink_hbm,
    route_hbm,
    share_hbm,
    x_hbm,
    gain_hbm,
    q_hbm,
    k_hbm,
    v_hbm,
    table_hbm,
    wg_hbm,
    wu_hbm,
    wd_hbm,
    mix_hbm,
    mixer_ref,
    expert_ref,
    sink,
    route_ref,
    share_ref,
    x_ref,
    gain_ref,
    q_ref,
    k_ref,
    v_ref,
    by_row,
    by_col,
    k_scr,
    v_scr,
    halo,
    att,
    att_in,
    routing,
    normed,
    picks,
    outgoing,
    arrived,
    produced,
    returned,
    shares,
    partial,
    home,
    relayed,
    relay_shares,
    relay_sum,
    relay_home,
    crossed,
    wg,
    wu,
    wd,
    mix,
    act,
    z_send,
    z_recv,
    rt_send,
    rt_recv,
    out_send,
    out_recv,
    back_send,
    back_recv,
    home_send,
    home_recv,
    relay_send,
    relay_recv,
    sum_send,
    sum_recv,
    cross_send,
    cross_recv,
    att_send,
    att_recv,
    halo_send,
    halo_recv,
    load_sem,
):
    n_z, n_x, n_y, n_tp, top_count, capacity = sizes
    n_ep = n_z * n_x
    plane = n_x * n_tp
    slots = plane * capacity
    cores = n_tp // n_y
    side = n_x * cores
    z, x, t = lax.axis_index("zz"), lax.axis_index("xx"), lax.axis_index("tp")
    me = x * n_tp + t
    y, core = lax.div(t, cores), lax.rem(t, cores)
    ep = z * n_x + x
    rows_here, width_q = q_ref.shape
    tok, width = x_ref.shape
    panel = width // PANELS
    back_width = [panel] * (PANELS - 1) + [panel - RELAYED]
    relay_cols = pl.ds(panel - RELAYED, RELAYED)
    length = rows_here * n_ep
    kv_local = k_scr.shape[0]
    bq = WINDOW
    span = bq + 2 * WINDOW
    blocks = rows_here // bq
    chunk = rows_here // n_tp
    last = n_z - 1
    grid_rows = by_row.shape[1]
    table_end = table_hbm.shape[1] - WINDOW

    def z_dev(b):
        return (b, x, t)

    def plane_dev(p):
        return (z, lax.div(p, n_tp), lax.rem(p, n_tp))

    def ep_dev(e):
        return (lax.div(e, n_x), lax.rem(e, n_x), t)

    after, before = lax.rem(ep + 1, n_ep), lax.rem(ep + n_ep - 1, n_ep)
    has_after, has_before = ep < n_ep - 1, ep > 0
    has_up, has_down = z < last, z > 0
    end = (z == 0) | (z == last)
    mid = (z > 0) & (z < last)

    closer = jnp.minimum(z, last - z)
    far_side = jnp.where(z < last - z, 1, -1)

    def nearest(i):
        if i == 0:
            return z
        paired = z + ((i + 1) // 2) * (-1 if i % 2 else 1)
        return jnp.where(i <= 2 * closer, paired, z + far_side * (i - closer))

    def going_back(i):
        return lax.bitwise_xor(z, jnp.int32(last - i))

    first_row = pl.multiple_of(ep * (rows_here // GRID_W), 8)
    loads = {
        "route": (route_hbm, route_ref),
        "share": (share_hbm, share_ref),
        "x": (x_hbm, x_ref),
        "gain": (gain_hbm, gain_ref),
        "sink": (sink_hbm, sink),
        "k": (k_hbm, k_ref),
        "v": (v_hbm, v_ref),
        "by_row": (table_hbm.at[:, pl.ds(first_row, grid_rows)], by_row),
        "by_col": (table_hbm.at[:, pl.ds(table_end, WINDOW)], by_col),
        "q": (q_hbm, q_ref),
        "wg": (wg_hbm.at[0], wg),
        "wu": (wu_hbm.at[0], wu),
        "wd": (wd_hbm.at[0], wd),
        "mix": (mix_hbm, mix),
    }
    loads = {
        name: pltpu.make_async_copy(source, target, load_sem.at[i])
        for i, (name, (source, target)) in enumerate(loads.items())
    }
    for load in loads.values():
        load.start()

    def loaded(*names):
        for name in names:
            loads[name].wait()

    barrier = pltpu.get_barrier_semaphore()

    def greet_z(o, _):
        pl.semaphore_signal(barrier, inc=1, device_id=z_dev(lax.rem(z + o, n_z)), device_id_type=MESH)
        return 0

    def greet_plane(p, _):
        pl.semaphore_signal(
            barrier, inc=1, device_id=plane_dev(lax.rem(me + p, plane)), device_id_type=MESH
        )
        return 0

    def column(o):
        b, row = lax.rem(z + o // n_y, n_z), lax.rem(y + o % n_y, n_y)
        return (b, x, row * cores + core)

    lax.fori_loop(1, n_z, greet_z, 0)
    for o in range(n_y + 1, n_z * n_y):
        if o % n_y:
            pl.semaphore_signal(barrier, inc=1, device_id=column(o), device_id_type=MESH)
    lax.fori_loop(1, plane, greet_plane, 0)
    for e in (after, before):
        pl.semaphore_signal(barrier, inc=1, device_id=ep_dev(e), device_id_type=MESH)

    def await_bytes(ref, sem):
        pltpu.make_async_copy(ref, ref, sem).wait()

    upper = (
        lax.broadcasted_iota(jnp.int32, (tok, tok), 0) < lax.broadcasted_iota(jnp.int32, (tok, tok), 1)
    ).astype(F32).astype(BF16)

    def pick_rows(route, expert_of_slot, count):
        slot_row = lax.broadcasted_iota(jnp.int32, (count, tok), 0)
        lane_expert = expert_of_slot(lax.div(slot_row, capacity)).astype(F32)
        place_in = lax.rem(slot_row, capacity).astype(F32)
        member = jnp.zeros((count, tok), F32)
        share = jnp.zeros((count, tok), F32)
        for k in range(top_count):
            hit = route[k : k + 1, :] == lane_expert
            member = jnp.where(hit, 1.0, member)
            share = jnp.where(hit, route[top_count + k : top_count + k + 1, :], share)
        rank = jnp.dot(member.astype(BF16), upper, preferred_element_type=F32)
        pick = jnp.where(rank == place_in, member, 0.0)
        scaled = (share * pick).T
        coarse = scaled.astype(BF16)
        return pick, coarse, (scaled - coarse.astype(F32)).astype(BF16)

    def choose(i):
        b = nearest(i)
        if i > 0:
            await_bytes(routing.at[b, y], rt_recv.at[b, y])
        pick, coarse, fine = pick_rows(routing[b, y], lambda e: z * plane + e, slots)
        picks[...] = pick.astype(BF16)
        shares[b, 0] = coarse
        shares[b, 1] = fine

    def choose_relayed(i):
        b = nearest(i)

        def expert(e):
            return z * plane + lax.div(e, cores) * n_tp + y * cores + lax.rem(e, cores)

        for o in range(n_y):
            row = lax.rem(y + o, n_y)
            if o > 0:
                await_bytes(routing.at[b, row], rt_recv.at[b, row])
            _, coarse, fine = pick_rows(routing[b, row], expert, side * capacity)
            relay_shares[b, row, 0] = coarse
            relay_shares[b, row, 1] = fine

    loaded("route", "share")
    routing[z, y, :top_count, :] = route_ref[...].astype(F32)
    routing[z, y, top_count:, :] = share_ref[...]
    choose(0)
    loaded("x", "gain")
    with scope("norm"):
        for part in range(tok // 32):
            rows = slice(part * 32, part * 32 + 32)
            values = x_ref[rows, :].astype(F32)
            center = jnp.mean(values, axis=1, keepdims=True)
            spread = jnp.mean(jnp.square(values - center), axis=1, keepdims=True)
            result = ((values - center) * lax.rsqrt(spread + NORM_EPS) * gain_ref[...]).astype(BF16)
            for h in range(PANELS):
                normed[z, h, rows, :] = result[:, h * panel : h * panel + panel]
    with scope("barr"):
        pl.semaphore_wait(barrier, (n_z - 1) * n_y + plane - 1 + 2)

    def rt_copy(o):
        return pltpu.make_async_remote_copy(
            src_ref=routing.at[z, y],
            dst_ref=routing.at[z, y],
            send_sem=rt_send.at[o],
            recv_sem=rt_recv.at[z, y],
            device_id=column(o),
            device_id_type=MESH,
        )

    def z_copy(i, h, b, target):
        return pltpu.make_async_remote_copy(
            src_ref=normed.at[b, h],
            dst_ref=normed.at[b, h],
            send_sem=z_send.at[i, h],
            recv_sem=z_recv.at[b, h],
            device_id=z_dev(target),
            device_id_type=MESH,
        )

    def onward(i):
        b = nearest(i)
        target = jnp.where(b < z, z + 1, z - 1)
        return b, target, (target >= 0) & (target <= last)

    for o in range(1, n_z * n_y):
        rt_copy(o).start()
    if n_z > 1:
        for h in range(PANELS):

            @pl.when(has_up)
            def _():
                z_copy(0, h, z, z + 1).start()

            @pl.when(has_down)
            def _():
                z_copy(n_z, h, z, z - 1).start()

    def tick(distance, h):
        for i in range(1, n_z):
            if not (i + 1) // 2 <= distance <= i:
                continue
            b, target, goes_on = onward(i)

            @pl.when(jnp.abs(b - z) == distance)
            def _():
                with scope(f"zwait{i}{h}"):
                    await_bytes(normed.at[b, h], z_recv.at[b, h])

                @pl.when(goes_on)
                def _():
                    z_copy(i, h, b, target).start()

    def dispatch(i, h):
        b = nearest(i)
        with scope(f"disp{i}{h}"):
            if h == 0 and i > 0:
                choose(i)

            def tile(j, _):
                cols = pl.ds(pl.multiple_of(j * TILE, TILE), TILE)
                outgoing[b, h, :, cols] = jnp.dot(
                    picks[...], normed[b, h, :, cols], preferred_element_type=F32
                ).astype(BF16)
                return 0

            parts = 2 if i == 0 and h == 0 else 1
            each = panel // parts
            for part in range(parts):
                lax.fori_loop(part * each // TILE, (part + 1) * each // TILE, tile, 0, unroll=i == 0)
                exchange(outgoing, arrived, out_send, out_recv, b, h, each, part * each)

    def exchange(source, target, send, recv, b, h, count, at=0):
        mine = pl.ds(pl.multiple_of(me * capacity, capacity), capacity)
        cols = pl.ds(at, count)

        def one(p, _):
            to = lax.rem(me + p, plane)
            pltpu.make_async_remote_copy(
                src_ref=source.at[b, h, pl.ds(pl.multiple_of(to * capacity, capacity), capacity), cols],
                dst_ref=target.at[b, h, mine, cols],
                send_sem=send.at[b, h],
                recv_sem=recv.at[b, h],
                device_id=plane_dev(to),
                device_id_type=MESH,
            ).start()
            return 0

        lax.fori_loop(1, plane, one, 0)
        pltpu.make_async_copy(
            source.at[b, h, mine, cols], target.at[b, h, mine, cols], recv.at[b, h]
        ).start()

    def halo_copy(source, which, start, target):
        return pltpu.make_async_remote_copy(
            src_ref=source.at[pl.ds(start, WINDOW)],
            dst_ref=halo.at[which],
            send_sem=halo_send.at[which],
            recv_sem=halo_recv.at[which],
            device_id=ep_dev(target),
            device_id_type=MESH,
        )

    to_after = [
        halo_copy(k_ref, 0, rows_here - WINDOW, after),
        halo_copy(v_ref, 1, rows_here - WINDOW, after),
    ]
    to_before = [halo_copy(k_ref, 2, 0, before), halo_copy(v_ref, 3, 0, before)]

    def send_halos():
        for there, copies in ((has_after, to_after), (has_before, to_before)):

            @pl.when(there)
            def _():
                for copy in copies:
                    copy.start()

    def await_halos():
        for there, copies in ((has_before, to_after), (has_after, to_before)):

            @pl.when(there)
            def _():
                for copy in copies:
                    copy.wait_recv()

        for there, which in ((has_before, 0), (has_after, 2)):

            @pl.when(jnp.logical_not(there))
            def _():
                halo[which] = jnp.zeros(halo.shape[1:], BF16)
                halo[which + 1] = jnp.zeros(halo.shape[1:], BF16)

    of_row = lax.rem(lax.broadcasted_iota(jnp.int32, (WINDOW, 128), 1), HEAD_DIM) < HEAD_DIM // 2

    def angles(which, at):
        start = lax.div(at, GRID_W)
        parts = [
            jnp.broadcast_to(by_row[which, pl.ds(start + i, 1), :], (GRID_W, 128))
            for i in range(WINDOW // GRID_W)
        ]
        return jnp.where(of_row, jnp.concatenate(parts, axis=0), by_col[which])

    def place(source, values, at, count):
        cosines, sines = angles(0, at), angles(1, at)
        for pair in range(kv_local // 2):
            cols = slice(pair * 128, pair * 128 + 128)
            turned = turn(source[:, cols].astype(F32), cosines, sines).astype(BF16)
            piece = values[:, cols]
            for side in range(2):
                lanes = slice(side * 64, side * 64 + 64)
                k_scr[2 * pair + side, pl.ds(at, count), :] = turned[:, lanes]
                v_scr[2 * pair + side, pl.ds(at, count), :] = piece[:, lanes]

    def place_own(i, _):
        at = pl.multiple_of(i * 128, 128)
        place(k_ref[pl.ds(at, 128), :], v_ref[pl.ds(at, 128), :], WINDOW + at, 128)
        return 0

    row = lax.rem(lax.broadcasted_iota(jnp.int32, (2 * bq, span), 0), bq)
    col = lax.broadcasted_iota(jnp.int32, (2 * bq, span), 1)
    top = lax.broadcasted_iota(jnp.int32, (2 * bq, 1), 0) < bq

    def attend(block, _):
        first = pl.multiple_of(block * bq, bq)
        cosines = angles(0, first + WINDOW) * HEAD_DIM**-0.5
        sines = angles(1, first + WINDOW) * HEAD_DIM**-0.5
        key_pos = ep * rows_here + first - WINDOW + col
        inside = (col >= row) & (col <= row + 2 * WINDOW) & (key_pos >= 0) & (key_pos < length)
        for g in range(kv_local):
            q = q_ref[pl.ds(first, bq), g * 128 : g * 128 + 128].astype(F32)
            q = turn(q, cosines, sines).astype(BF16)
            q2 = jnp.concatenate([q[:, :64], q[:, 64:]], axis=0)
            k = k_scr[g, pl.ds(first, span), :]
            v = v_scr[g, pl.ds(first, span), :]
            scores = lax.dot_general(q2, k, (((1,), (1,)), ((), ())), preferred_element_type=F32)
            scores = jnp.where(inside, scores, -jnp.inf)
            logit = jnp.where(top, sink[2 * g], sink[2 * g + 1])
            peak = jnp.maximum(jnp.max(scores, axis=1, keepdims=True), logit)
            weights = jnp.exp(scores - peak)
            total = jnp.sum(weights, axis=1, keepdims=True) + jnp.exp(logit - peak)
            chances = (weights * (1.0 / total)).astype(BF16)
            blend = jnp.dot(chances, v, preferred_element_type=F32).astype(BF16)
            att[pl.ds(first, bq), g * 128 : g * 128 + 128] = jnp.concatenate(
                [blend[:bq], blend[bq:]], axis=1
            )
        return 0

    def attend_inner(part, parts):
        inner = blocks - 2
        with scope(f"att{part}"):
            lax.fori_loop(1 + inner * part // parts, 1 + inner * (part + 1) // parts, attend, 0)

    def attend_edges():
        with scope("halowait"):
            await_halos()
        with scope("edges"):
            place(halo[0], halo[1], 0, WINDOW)
            place(halo[2], halo[3], WINDOW + rows_here, WINDOW)
            lax.fori_loop(0, 2, lambda i, _: attend(i * (blocks - 1), _), 0)

    def send_heads(edges):
        each = chunk // bq

        def one(p, _):
            to = lax.rem(t + p, n_tp)
            for i in range(each):
                block = to * each + i
                at_edge = (block == 0) | (block == blocks - 1)

                @pl.when(at_edge if edges else jnp.logical_not(at_edge))
                def _():
                    pltpu.make_async_remote_copy(
                        src_ref=att.at[pl.ds(pl.multiple_of(block * bq, bq), bq)],
                        dst_ref=att_in.at[t, i * bq : i * bq + bq],
                        send_sem=att_send,
                        recv_sem=att_recv,
                        device_id=(z, x, to),
                        device_id_type=MESH,
                    ).start()

            return 0

        lax.fori_loop(1, n_tp, one, 0)
        if edges:
            own = pl.ds(pl.multiple_of(t * chunk, chunk), chunk)
            pltpu.make_async_copy(att.at[own], att_in.at[t], att_recv).start()

    def mixer():
        with scope("attwait"):
            await_bytes(att_in, att_recv)
        loaded("mix")

        def tile(j, _):
            cols = pl.ds(pl.multiple_of(j * TILE, TILE), TILE)
            total = jnp.zeros((chunk, TILE), F32)
            for s in range(n_tp):
                total = total + jnp.dot(
                    att_in[s], mix[s * width_q : s * width_q + width_q, cols], preferred_element_type=F32
                )
            mixer_ref[:, cols] = total.astype(BF16)
            return 0

        with scope("mixer"):
            lax.fori_loop(0, width // TILE, tile, 0)

    def experts(i, sent=lambda h: None):
        b = nearest(i)
        hidden = wg.shape[1]
        for h in range(PANELS):
            with scope(f"arrwait{i}{h}"):
                await_bytes(arrived.at[b, h], out_recv.at[b, h])

        def up(j, _):
            cols = pl.ds(pl.multiple_of(j * TILE, TILE), TILE)
            gate = jnp.zeros((slots, TILE), F32)
            lift = jnp.zeros((slots, TILE), F32)
            for h in range(PANELS):
                rows = arrived[b, h]
                deep = slice(h * panel, h * panel + panel)
                gate = gate + jnp.dot(rows, wg[deep, cols], preferred_element_type=F32)
                lift = lift + jnp.dot(rows, wu[deep, cols], preferred_element_type=F32)
            gate = jnp.minimum(gate, CLAMP_LIMIT)
            lift = jnp.clip(lift, -CLAMP_LIMIT, CLAMP_LIMIT)
            act[:, cols] = ((lift + 1.0) * gate * jax.nn.sigmoid(GATE_SLOPE * gate)).astype(BF16)
            return 0

        with scope(f"exp{i}"):
            lax.fori_loop(0, hidden // TILE, up, 0)
            for h in range(PANELS):

                def down(j, _):
                    cols = pl.ds(pl.multiple_of(j * TILE, TILE), TILE)
                    wide = pl.ds(pl.multiple_of(h * panel + j * TILE, TILE), TILE)
                    produced[b, h, :, cols] = jnp.dot(
                        act[...], wd[:, wide], preferred_element_type=F32
                    ).astype(BF16)
                    return 0

                lax.fori_loop(0, panel // TILE, down, 0)
                sent(h)

    def send_back(b, h):
        exchange(produced, returned, back_send, back_recv, b, h, back_width[h])

    def send_relayed(b):
        mine = pl.ds(pl.multiple_of((x * cores + core) * capacity, capacity), capacity)

        def source(to, row):
            slot = lax.div(to, cores) * n_tp + row * cores + lax.rem(to, cores)
            rows = pl.ds(pl.multiple_of(slot * capacity, capacity), capacity)
            return produced.at[b, PANELS - 1, rows, relay_cols]

        def one(p, _):
            to = lax.rem(x * cores + core + p, side)
            for row in range(n_y):
                pltpu.make_async_remote_copy(
                    src_ref=source(to, row),
                    dst_ref=relayed.at[b, row, mine],
                    send_sem=relay_send.at[b],
                    recv_sem=relay_recv.at[b],
                    device_id=(z, lax.div(to, cores), y * cores + lax.rem(to, cores)),
                    device_id_type=MESH,
                ).start()
            return 0

        lax.fori_loop(1, side, one, 0)
        for row in range(n_y):
            pltpu.make_async_copy(
                source(x * cores + core, row), relayed.at[b, row, mine], relay_recv.at[b]
            ).start()

    def homeward(b):
        target = jnp.where(b < z, z - 1, z + 1)
        return target, jnp.where((target == b) & (b < z), n_z, b)

    def home_copy(b, h):
        target, slot = homeward(b)
        cols = pl.ds(0, back_width[h])
        return pltpu.make_async_remote_copy(
            src_ref=partial.at[b, h, :, cols],
            dst_ref=home.at[slot, h, :, cols],
            send_sem=home_send.at[b, h],
            recv_sem=home_recv.at[slot, h],
            device_id=z_dev(target),
            device_id_type=MESH,
        )

    def relay_copy(b):
        target, slot = homeward(b)
        return pltpu.make_async_remote_copy(
            src_ref=relay_sum.at[b],
            dst_ref=relay_home.at[slot],
            send_sem=sum_send.at[b],
            recv_sem=sum_recv.at[slot],
            device_id=z_dev(target),
            device_id_type=MESH,
        )

    def cross_copy(o):
        row = lax.rem(y + o, n_y)
        return pltpu.make_async_remote_copy(
            src_ref=relay_sum.at[z, row],
            dst_ref=crossed.at[y],
            send_sem=cross_send.at[o],
            recv_sem=cross_recv.at[y],
            device_id=(z, x, row * cores + core),
            device_id_type=MESH,
        )

    def clear_home():
        for slot, missing in ((z, z == 0), (n_z, z == last)):

            @pl.when(missing)
            def _():
                home[slot] = jnp.zeros(home.shape[1:], BF16)
                relay_home[slot] = jnp.zeros(relay_home.shape[1:], BF16)

    def weighted(b, h, cols):
        rows = returned[b, h, :, cols]
        total = jnp.dot(shares[b, 0], rows, preferred_element_type=F32)
        return total + jnp.dot(shares[b, 1], rows, preferred_element_type=F32)

    def relay_weighted(b, row):
        rows = relayed[b, row]
        total = jnp.dot(relay_shares[b, row, 0], rows, preferred_element_type=F32)
        return total + jnp.dot(relay_shares[b, row, 1], rows, preferred_element_type=F32)

    def combine_relayed(name, b, further):
        with scope(f"relwait{name}"):
            await_bytes(relayed.at[b], relay_recv.at[b])
            if further:
                await_bytes(relay_home.at[b], sum_recv.at[b])

        with scope(f"rel{name}"):
            for row in range(n_y):
                total = relay_weighted(b, row)
                if further:
                    total = total + relay_home[b, row].astype(F32)
                relay_sum[b, row] = total.astype(BF16)
        relay_copy(b).start()

    def from_both_sides(place, sem):
        @pl.when(has_down)
        def _():
            await_bytes(place(z), sem(z))

        @pl.when(has_up)
        def _():
            await_bytes(place(n_z), sem(n_z))

    def combine_own_relayed():
        with scope("relwaitown"):
            await_bytes(relayed.at[z], relay_recv.at[z])
            from_both_sides(lambda slot: relay_home.at[slot], lambda slot: sum_recv.at[slot])
        for row in range(n_y):
            total = relay_weighted(z, row) + relay_home[z, row].astype(F32)
            relay_sum[z, row] = (total + relay_home[n_z, row].astype(F32)).astype(BF16)
        for o in range(1, n_y):
            cross_copy(o).start()

    def finish_relayed():
        total = relay_sum[z, y].astype(F32)
        for o in range(1, n_y):
            row = lax.rem(y + o, n_y)
            with scope("crosswait"):
                await_bytes(crossed.at[row], cross_recv.at[row])
            total = total + crossed[row].astype(F32)
        expert_ref[:, width - RELAYED :] = total.astype(BF16)

    def combine(name, b, h, further):
        cols = pl.ds(0, back_width[h])
        with scope(f"retwait{name}"):
            await_bytes(returned.at[b, h, :, cols], back_recv.at[b, h])

        if further:
            with scope(f"chain{name}"):
                await_bytes(home.at[b, h, :, cols], home_recv.at[b, h])

        def tile(j, _):
            cols = pl.ds(pl.multiple_of(j * TILE, TILE), TILE)
            total = weighted(b, h, cols)
            if further:
                total = total + home[b, h, :, cols].astype(F32)
            partial[b, h, :, cols] = total.astype(BF16)
            return 0

        with scope(f"comb{name}"):
            lax.fori_loop(0, back_width[h] // TILE, tile, 0)
        home_copy(b, h).start()

    def combine_own(h):
        here = pl.ds(0, back_width[h])
        with scope(f"retwaitown{h}"):
            await_bytes(returned.at[z, h, :, here], back_recv.at[z, h])
        with scope(f"homewait{h}"):
            from_both_sides(lambda slot: home.at[slot, h, :, here], lambda slot: home_recv.at[slot, h])

        def tile(j, _):
            cols = pl.ds(pl.multiple_of(j * TILE, TILE), TILE)
            wide = pl.ds(pl.multiple_of(h * panel + j * TILE, TILE), TILE)
            total = weighted(z, h, cols) + home[z, h, :, cols].astype(F32)
            total = total + home[n_z, h, :, cols].astype(F32)
            expert_ref[:, wide] = total.astype(BF16)
            return 0

        with scope(f"combown{h}"):
            lax.fori_loop(0, back_width[h] // TILE, tile, 0, unroll=True)

    for h in range(PANELS):
        dispatch(0, h)
    clear_home()
    loaded("k", "v", "by_row", "by_col", "q", "sink")
    with scope("place"):
        lax.fori_loop(0, rows_here // 128, place_own, 0)
    attend_inner(0, 3)
    for h in range(PANELS):
        if n_z > 1:
            tick(1, h)
            dispatch(1, h)
        attend_inner(1 + h, 3)
    if n_z > 2:
        tick(2, 0)
        dispatch(2, 0)
    loaded("wg", "wu", "wd")
    if n_z > 1:
        experts(0)
    if n_z > 2:
        tick(2, 1)
        dispatch(2, 1)
        experts(1)
        for h in range(PANELS):
            tick(3, h)
            dispatch(3, h)
    send_halos()
    send_heads(False)
    if n_z > 1:
        send_relayed(z)
    if n_z > 2:
        send_relayed(nearest(1))
    with scope("chooserel"):
        for i in range(n_z):
            choose_relayed(i)
    if n_z > 2:
        experts(2)
        send_relayed(nearest(2))

        @pl.when(mid)
        def _():
            for h in range(PANELS):
                send_back(going_back(0), h)

    def sent(h):
        if h == PANELS - 1:
            send_relayed(nearest(last))

        @pl.when(end)
        def _():
            send_back(going_back(0), h)

    def sums(steps, further=False):
        for i, h in steps:
            if h is None:
                combine_relayed(i, going_back(i), further)
            else:
                combine(f"{i}{h}", going_back(i), h, further)

    def all_of(i):
        return [(i, h) for h in range(PANELS)]

    experts(last, sent)
    if n_z > 2:

        @pl.when(end)
        def _():
            sums([(2, None), (1, None)])

    attend_edges()
    send_heads(True)
    for i in range(1, n_z):
        for h in range(PANELS if i < last else PANELS - 1):
            send_back(going_back(i), h)
    if n_z > 2:

        @pl.when(end)
        def _():
            sums([(0, None)] + all_of(0))
            mixer()
            sums(all_of(1))

        @pl.when(mid)
        def _():
            sums([(0, None), (1, None)], True)
            mixer()
            sums([(2, None)] + all_of(1), True)
    else:
        if n_z > 1:
            sums([(0, None)] + all_of(0))
        mixer()
    combine_own_relayed()
    if n_z > 1:
        send_back(z, PANELS - 1)
    if n_z > 2:

        @pl.when(end)
        def _():
            sums(all_of(2))

        @pl.when(mid)
        def _():
            sums([(i, h) for h in range(PANELS) for i in (2, 0)], True)

    for o in range(1, n_z * n_y):
        rt_copy(o).wait_send()
    if n_z > 1:
        for h in range(PANELS):

            @pl.when(has_up)
            def _():
                z_copy(0, h, z, z + 1).wait_send()

            @pl.when(has_down)
            def _():
                z_copy(n_z, h, z, z - 1).wait_send()

            for i in range(1, n_z):
                b, target, goes_on = onward(i)

                @pl.when(goes_on)
                def _():
                    z_copy(i, h, b, target).wait_send()
    for there, copies in ((has_after, to_after), (has_before, to_before)):

        @pl.when(there)
        def _():
            for copy in copies:
                copy.wait_send()

    for b in range(n_z):
        for h in range(PANELS):
            gone = pl.ds(0, (plane - 1) * capacity)
            await_bytes(outgoing.at[b, h, gone], out_send.at[b, h])
        gone = pl.ds(0, (side - 1) * n_y * capacity)
        await_bytes(produced.at[b, 0, gone, pl.ds(0, RELAYED)], relay_send.at[b])
    await_bytes(att.at[pl.ds(0, (n_tp - 1) * chunk)], att_send)

    for h in range(PANELS):
        combine_own(h)
        if h == 0:
            finish_relayed()

    with scope("late"):
        for h in range(PANELS):
            for i in range(1, n_z):
                home_copy(nearest(i), h).wait_send()
            for b in range(n_z):
                gone = pl.ds(0, (plane - 1) * capacity)
                await_bytes(produced.at[b, h, gone, pl.ds(0, back_width[h])], back_send.at[b, h])
        for i in range(1, n_z):
            relay_copy(nearest(i)).wait_send()
        for o in range(1, n_y):
            cross_copy(o).wait_send()


def hand_over(mixer_in, expert_in, mixer_out, expert_out, sem):
    copies = [
        pltpu.make_async_copy(source, target, sem.at[i])
        for i, (source, target) in enumerate(((mixer_in, mixer_out), (expert_in, expert_out)))
    ]
    for copy in copies:
        copy.start()
    for copy in copies:
        copy.wait()


def body(
    n_y,
    queries,
    key_heads,
    value_heads,
    sink_logits,
    mix_weight,
    expert_input,
    norm_gain,
    routes,
    route_weights,
    gate_weight,
    up_weight,
    down_weight,
):
    n_z, n_x, n_tp = lax.axis_size("zz"), lax.axis_size("xx"), lax.axis_size("tp")
    n_ep = n_z * n_x
    plane = n_x * n_tp
    rows_here, width_q = queries.shape
    kv_width = key_heads.shape[1]
    kv_local = kv_width // HEAD_DIM
    tok, top_count = routes.shape
    capacity = 2 * tok * top_count // (n_ep * n_tp)
    slots = plane * capacity
    width = expert_input.shape[1]
    panel = width // PANELS
    hidden = gate_weight.shape[2]
    tables = jnp.asarray(angle_tables(rows_here * n_ep, rows_here))
    anywhere = pl.BlockSpec(memory_space=pl.ANY)
    vmem = pl.BlockSpec(memory_space=pltpu.VMEM)
    reach = rows_here + 2 * WINDOW
    dma = pltpu.SemaphoreType.DMA
    shapes = [
        jax.ShapeDtypeStruct((rows_here // n_tp, width), BF16),
        jax.ShapeDtypeStruct((tok, width), BF16),
    ]
    both = dma((n_z, PANELS))
    side_slots = slots // n_y
    mixed, expert = pl.pallas_call(
        functools.partial(kernel, (n_z, n_x, n_y, n_tp, top_count, capacity)),
        in_specs=[anywhere] * 13,
        out_specs=[vmem] * 2,
        out_shape=[pltpu.VMEM(s.shape, s.dtype) for s in shapes],
        scratch_shapes=[
            pltpu.SMEM(sink_logits.shape, F32),
            pltpu.VMEM((top_count, tok), jnp.int32),
            pltpu.VMEM((top_count, tok), F32),
            pltpu.VMEM((tok, width), BF16),
            pltpu.VMEM((1, width), F32),
            pltpu.VMEM((rows_here, width_q), BF16),
            pltpu.VMEM((rows_here, kv_width), BF16),
            pltpu.VMEM((rows_here, kv_width), BF16),
            pltpu.VMEM((2, table_rows(rows_here), 128), F32),
            pltpu.VMEM((2, WINDOW, 128), F32),
            pltpu.VMEM((kv_local, reach, HEAD_DIM), BF16),
            pltpu.VMEM((kv_local, reach, HEAD_DIM), BF16),
            pltpu.VMEM((4, WINDOW, kv_width), BF16),
            pltpu.VMEM((rows_here, width_q), BF16),
            pltpu.VMEM((n_tp, rows_here // n_tp, width_q), BF16),
            pltpu.VMEM((n_z, n_y, 2 * top_count, tok), F32),
            pltpu.VMEM((n_z, PANELS, tok, panel), BF16),
            pltpu.VMEM((slots, tok), BF16),
            pltpu.VMEM((n_z, PANELS, slots, panel), BF16),
            pltpu.VMEM((n_z, PANELS, slots, panel), BF16),
            pltpu.VMEM((n_z, PANELS, slots, panel), BF16),
            pltpu.VMEM((n_z, PANELS, slots, panel), BF16),
            pltpu.VMEM((n_z, 2, tok, slots), BF16),
            pltpu.VMEM((n_z, PANELS, tok, panel), BF16),
            pltpu.VMEM((n_z + 1, PANELS, tok, panel), BF16),
            pltpu.VMEM((n_z, n_y, side_slots, RELAYED), BF16),
            pltpu.VMEM((n_z, n_y, 2, tok, side_slots), BF16),
            pltpu.VMEM((n_z, n_y, tok, RELAYED), BF16),
            pltpu.VMEM((n_z + 1, n_y, tok, RELAYED), BF16),
            pltpu.VMEM((n_y, tok, RELAYED), BF16),
            pltpu.VMEM((width, hidden), BF16),
            pltpu.VMEM((width, hidden), BF16),
            pltpu.VMEM((hidden, width), BF16),
            pltpu.VMEM(mix_weight.shape, BF16),
            pltpu.VMEM((slots, hidden), BF16),
            dma((n_z + 1, PANELS)),
            both,
            dma((n_z * n_y,)),
            dma((n_z, n_y)),
            both,
            both,
            both,
            both,
            both,
            dma((n_z + 1, PANELS)),
            dma((n_z,)),
            dma((n_z,)),
            dma((n_z,)),
            dma((n_z + 1,)),
            dma((n_y,)),
            dma((n_y,)),
            dma,
            dma,
            dma((4,)),
            dma((4,)),
            dma((14,)),
        ],
        compiler_params=pltpu.CompilerParams(
            collective_id=0, has_side_effects=True, vmem_limit_bytes=VMEM_BYTES
        ),
        name="layer",
    )(
        sink_logits,
        routes.T,
        route_weights.T,
        expert_input,
        norm_gain[None, :],
        queries,
        key_heads,
        value_heads,
        tables,
        gate_weight,
        up_weight,
        down_weight,
        mix_weight,
    )
    return pl.pallas_call(
        hand_over,
        in_specs=[vmem] * 2,
        out_specs=[anywhere] * 2,
        out_shape=shapes,
        scratch_shapes=[dma((2,))],
        name="hand_over",
    )(
        pltpu.with_memory_space_constraint(mixed, pltpu.VMEM),
        pltpu.with_memory_space_constraint(expert, pltpu.VMEM),
    )


def count_of(mesh, axis, among):
    coords = {getattr(d, "coords", (0, 0, 0))[axis] for d in mesh.devices.flat}
    return len(coords) if among % len(coords) == 0 else 1


def solution(mesh):
    n_ep, n_tp = mesh.shape["ep"], mesh.shape["tp"]
    n_z, n_y = count_of(mesh, 2, n_ep), count_of(mesh, 1, n_tp)
    n_z = n_z if n_z in (1, 2, 4) else 1
    grid = Mesh(mesh.devices.reshape(n_z, n_ep // n_z, n_tp), ("zz", "xx", "tp"))
    ep = ("zz", "xx")
    every = ("zz", "xx", "tp")
    return jax.shard_map(
        functools.partial(body, n_y),
        mesh=grid,
        in_specs=(
            P(ep, "tp"),
            P(ep, "tp"),
            P(ep, "tp"),
            P("tp"),
            P(),
            P(every, None),
            P(),
            P(every, None),
            P(every, None),
            P(every, None, None),
            P(every, None, None),
            P(every, None, None),
        ),
        out_specs=(P(every, None), P(every, None)),
        check_vma=False,
    )
```
